32 devices in a mesh: sp: 16 (over z, y, x), tp: 2 (over core).
Axes of the slice: x: 2, y: 2, z: 4, core: 2. Of those that a mesh axis runs over, the one named last changes fastest.
Arguments:
- queries: bfloat16 [4096, 512], P('sp', 'tp'), may hold values from -6 to 6
- keys: bfloat16 [4096, 512], P('sp', 'tp'), may hold values from -6 to 6
- values: bfloat16 [4096, 512], P('sp', 'tp'), may hold values from -6 to 6
- gains: float32 [2, 128], replicated, may hold values from 0.1 to 1.9
- bias_table: float32 [192, 4], P(None, 'tp'), may hold values from -6 to 270
- d_out: bfloat16 [4096, 512], P('sp', 'tp'), may hold values from -32 to 32
Outputs:
- d_queries: bfloat16 [4096, 512], P('sp', 'tp')
- d_keys: bfloat16 [4096, 512], P('sp', 'tp')
- d_values: bfloat16 [4096, 512], P('sp', 'tp')
- d_table: float32 [192, 4], P(None, 'tp')
- d_gains: float32 [2, 128], replicated
The draws below stay inside these ranges and needn't reach their ends.
All inputs are finite; a program needn't handle non-finite values.
Results may differ from the reference program's by a relative error of at most 0.008.
Values may be sent and summed in bfloat16 or wider, within the bound.
No kernel may reach another device: no remote copies, remote signals or barrier semaphores. Data moves between devices by JAX's collectives and lax.ppermute only.
A program may use at most 64 MiB of HBM per device.

```python
import jax
import jax.numpy as jnp
from jax import lax

HEADS = 4
HEAD_DIM = 128
SEG = 64
LEFT = 4
MAX_REL = 128
TOKENS = 4096


def draw_bias_table(key, part):
    entries = MAX_REL + SEG
    rough = jnp.clip(jax.random.normal(key, (entries, HEADS), jnp.float32), -6.0, 6.0)
    return rough.astype(jnp.float32)


def draw_d_out(key, part):
    width = HEADS * HEAD_DIM
    position = jnp.arange(TOKENS).astype(jnp.float32)[:, None] / TOKENS
    spread = 10.0 ** (jax.random.uniform(jax.random.fold_in(key, 1), (TOKENS, 1), jnp.float32) - 1.0)
    base = jnp.clip(jax.random.normal(jax.random.fold_in(key, 2), (TOKENS, width), jnp.float32), -6.0, 6.0)
    rise = 3.0 ** position
    return (base * spread * rise).astype(jnp.bfloat16)


def shard_levels(own_key, dims, shards, smallest, high):
    gain = 1.0
    for axis_at, shards_of in shards:
        heights = jax.random.uniform(jax.random.fold_in(jax.random.fold_in(own_key, 6), axis_at), (shards_of,), jnp.float32, smallest / len(shards), high / len(shards))
        gain = gain * jnp.repeat(jnp.exp(heights), dims[axis_at] // shards_of).reshape((-1,) + (1,) * (len(dims) - 1 - axis_at))
    return gain


def centred(own_key, shape, scale, bound, cuts=(), held_as=jnp.bfloat16):
    values = scale * jax.random.normal(own_key, shape, jnp.float32)
    if cuts:
        values = values * shard_levels(own_key, shape, cuts, -0.22, 0.18)
    return jnp.clip(values, -bound, bound).astype(held_as)


def setup_inputs(seed: int = 0) -> dict:
    streams_of = jax.random.split(jax.random.key(seed), 7)
    return {
        "queries": centred(streams_of[0], (TOKENS, HEADS * HEAD_DIM), 1.0, 6.0, ((0, 16), (1, 2))),
        "keys": centred(streams_of[1], (TOKENS, HEADS * HEAD_DIM), 1.0, 6.0, ((0, 16), (1, 2))),
        "values": centred(streams_of[2], (TOKENS, HEADS * HEAD_DIM), 1.0, 6.0, ((0, 16), (1, 2))),
        "gains": jnp.clip(1.0 + 0.18 * jax.random.normal(streams_of[3], (2, HEAD_DIM), jnp.float32), 0.1, 1.9),
        "bias_table": draw_bias_table(jax.random.fold_in(streams_of[6], 71), 0),
        "d_out": draw_d_out(jax.random.fold_in(streams_of[6], 71), 0),
    }


EPSILON = 1e-06

def unit_rows(row_block):
    widened = row_block.astype(jnp.float32).reshape(row_block.shape[0], HEADS, HEAD_DIM)
    inv_rms = lax.rsqrt(lax.optimization_barrier(jnp.mean(widened * widened, axis=-1, keepdims=True)) + EPSILON)
    return (widened * inv_rms, inv_rms)

def rows_back(d_normed, row_block, gain_vec):
    unit_part, inv_rms = unit_rows(row_block)
    d_unit = d_normed * gain_vec
    d_rows = inv_rms * (d_unit - unit_part * lax.optimization_barrier(jnp.mean(d_unit * unit_part, axis=-1, keepdims=True)))
    return (d_rows.reshape(row_block.shape[0], -1).astype(jnp.bfloat16), lax.optimization_barrier(jnp.sum(d_normed * unit_part, axis=(0, 1))))

def lowered(array_in):
    return lax.optimization_barrier(array_in.astype(jnp.bfloat16)).astype(jnp.float32)

def reference(queries, keys, values, gains, bias_table, d_out):
    tail_rows = LEFT * SEG
    blocks = TOKENS // tail_rows
    factor = HEAD_DIM ** (-0.5)
    q_unit, _ = unit_rows(queries)
    q_norm = (q_unit * gains[0]).astype(jnp.bfloat16)
    k_unit, _ = unit_rows(keys)
    k_norm = (k_unit * gains[1]).astype(jnp.bfloat16)
    leading = jnp.zeros((tail_rows, HEADS, HEAD_DIM), jnp.bfloat16)
    k_all = jnp.concatenate([leading, k_norm])
    v_all = jnp.concatenate([leading, values.reshape(TOKENS, HEADS, HEAD_DIM)])
    q_blocks = q_norm.reshape(blocks, tail_rows, HEADS, HEAD_DIM)
    do_blocks = d_out.reshape(blocks, tail_rows, HEADS, HEAD_DIM)
    query_idx = jnp.arange(tail_rows, dtype=jnp.int32)[:, None]
    key_idx = jnp.arange(2 * tail_rows, dtype=jnp.int32)[None, :]
    rel_index = (jnp.clip(query_idx + tail_rows - key_idx, -(SEG - 1), MAX_REL) + SEG - 1).astype(jnp.int32)
    bias_tiles = jnp.transpose(bias_table[rel_index], (2, 0, 1))
    flat_index = rel_index.reshape(-1)

    def advance(state, entry):
        pend_k, pend_v, table_sum = state
        number, q_block, do_block = entry
        start = number * tail_rows
        k_ext = lax.dynamic_slice_in_dim(k_all, start, 2 * tail_rows, 0).astype(jnp.float32)
        v_ext = lax.dynamic_slice_in_dim(v_all, start, 2 * tail_rows, 0).astype(jnp.float32)
        query_seg = (start + query_idx) // SEG
        key_pos = start - tail_rows + key_idx
        key_seg = key_pos // SEG
        key_valid = (key_pos >= 0) & (key_seg >= query_seg - LEFT) & (key_seg <= query_seg)
        q_float = q_block.astype(jnp.float32)
        do_float = do_block.astype(jnp.float32)
        scores = jnp.einsum('ihd,jhd->hij', q_float, k_ext) * factor + bias_tiles
        scores = jnp.where(key_valid[None], scores, -jnp.inf)
        row_max = lax.optimization_barrier(jnp.max(scores, axis=-1, keepdims=True))
        log_total = row_max + jnp.log(lax.optimization_barrier(jnp.sum(jnp.exp(scores - row_max), axis=-1, keepdims=True)))
        prob = jnp.exp(scores - log_total)
        d_prob = jnp.einsum('ihd,jhd->hij', do_float, v_ext)
        row_delta = lax.optimization_barrier(jnp.sum(prob * d_prob, axis=-1, keepdims=True))
        d_score = prob * (d_prob - row_delta)
        prob_low = lowered(prob)
        d_low = lowered(d_score)
        grad_v = jnp.einsum('hij,ihd->jhd', prob_low, do_float)
        grad_k = jnp.einsum('hij,ihd->jhd', d_low, q_float) * factor
        grad_q = jnp.einsum('hij,jhd->ihd', d_low, k_ext) * factor
        table_part = jax.ops.segment_sum(jnp.transpose(d_score, (1, 2, 0)).reshape(-1, HEADS), flat_index, num_segments=MAX_REL + SEG)
        emitted = (pend_k + grad_k[:tail_rows], pend_v + grad_v[:tail_rows], grad_q)
        return ((grad_k[tail_rows:], grad_v[tail_rows:], table_sum + table_part), emitted)
    zero_rows = jnp.zeros((tail_rows, HEADS, HEAD_DIM), jnp.float32)
    initial = (zero_rows, zero_rows, jnp.zeros((MAX_REL + SEG, HEADS), jnp.float32))
    numbers = jnp.arange(blocks, dtype=jnp.int32)
    (last_k, last_v, d_table), (ys_k, ys_v, ys_q) = lax.scan(advance, initial, (numbers, q_blocks, do_blocks))
    d_kn = jnp.concatenate([ys_k[1:].reshape(-1, HEADS, HEAD_DIM), last_k])
    d_vn = jnp.concatenate([ys_v[1:].reshape(-1, HEADS, HEAD_DIM), last_v])
    d_qn = ys_q.reshape(TOKENS, HEADS, HEAD_DIM)
    d_queries, gain_q = rows_back(d_qn, queries, gains[0])
    d_keys, gain_k = rows_back(d_kn, keys, gains[1])
    d_values = d_vn.reshape(TOKENS, -1).astype(jnp.bfloat16)
    return (d_queries, d_keys, d_values, d_table, jnp.stack([gain_q, gain_k]))
```

```python
import functools

import jax
import jax.numpy as jnp
from jax import lax
from jax.experimental import pallas as pl
from jax.experimental.pallas import tpu as pltpu
from jax.sharding import PartitionSpec as P

HEAD_DIM = 128
SEG = 64
LEFT = 4
MAX_REL = 128
ENTRIES = MAX_REL + SEG
EPSILON = 1e-06
FACTOR = HEAD_DIM ** (-0.5)
TAIL = LEFT * SEG

BLOCK = 2 * SEG
WINDOW = LEFT // 2 + 1
MASKED = -1e30

F32 = jnp.float32
BF16 = jnp.bfloat16


def dot(a, b, contract):
    return lax.dot_general(a, b, ((contract[:1], contract[1:]), ((), ())), preferred_element_type=F32)


def shifted(block, distance):
    devices = range(lax.axis_size("sp"))
    route = [(i - distance, i) for i in devices if i - distance in devices]
    return lax.ppermute(block, "sp", route)


def unit_rows(rows):
    rows = rows.astype(F32)
    inv_rms = lax.rsqrt(jnp.mean(rows * rows, axis=-1, keepdims=True) + EPSILON)
    return rows * inv_rms, inv_rms


def rows_back(d_normed, unit, inv_rms, gain):
    g = d_normed * gain
    return inv_rms * (g - unit * jnp.mean(g * unit, axis=-1, keepdims=True))


def lanes(shape):
    return lax.broadcasted_iota(jnp.int32, shape, len(shape) - 1)


def toeplitz(row):
    base = pltpu.roll(jnp.broadcast_to(row, (8, 2 * BLOCK)), 0, 1, stride=1, stride_axis=0)
    tiles = [base[:, :BLOCK]]
    for a in range(8, BLOCK, 8):
        tiles.append(pltpu.roll(base, a, 1)[:, :BLOCK])
    return jnp.concatenate(tiles, axis=0)


def diagonals(tile):
    width = 2 * BLOCK
    total = jnp.zeros((8, width), F32)
    empty = jnp.zeros((8, BLOCK), F32)
    for a in range(0, BLOCK, 8):
        part = jnp.concatenate([tile[a : a + 8], empty], axis=1)
        total = total + (pltpu.roll(part, width - a, 1) if a else part)
    out = total[:1]
    for s in range(1, 8):
        out = out + pltpu.roll(total, width - s, 1)[s : s + 1]
    return out


def bias_blocks(table):
    width = 2 * BLOCK
    last = table[:, ENTRIES - 1 :]
    lane = lanes((1, width))
    wide = jnp.concatenate([table, jnp.zeros((1, width - ENTRIES), F32)], axis=1)
    far = jnp.broadcast_to(last, (BLOCK, BLOCK))
    middle = toeplitz(jnp.where(lane < BLOCK, last, pltpu.roll(wide, width - (ENTRIES - 1), 1)))
    near = toeplitz(pltpu.roll(wide, width - (SEG - 1), 1))
    key = lax.broadcasted_iota(jnp.int32, (BLOCK, BLOCK), 0)
    query = lax.broadcasted_iota(jnp.int32, (BLOCK, BLOCK), 1)
    far = jnp.where((key < SEG) & (query >= SEG), MASKED, far)
    near = jnp.where((key >= SEG) & (query < SEG), MASKED, near)
    return [far, middle, near]


def table_row(far, middle, near):
    width = 2 * BLOCK
    lane = lanes((1, width))
    mid = diagonals(middle)
    last = jnp.sum(far) + jnp.sum(jnp.where(lane < BLOCK, mid, 0.0))
    mid = jnp.where(lane < BLOCK, 0.0, mid)
    row = pltpu.roll(diagonals(near), SEG - 1, 1) + pltpu.roll(mid, ENTRIES - 1, 1)
    return row + jnp.where(lane == ENTRIES - 1, last, 0.0)


def band_kernel(
    q_ref, k_ref, v_ref, do_ref, pk_ref, pv_ref, gains_ref, table_ref,
    dq_ref, back_ref, own_ref, parts_ref,
):
    rows, features = q_ref.shape
    heads = features // HEAD_DIM
    blocks = rows // BLOCK
    first = lax.axis_index("sp") == 0
    gain_q = gains_ref[0:1]
    gain_k = gains_ref[1:2]
    pieces = []
    d_gain_q = jnp.zeros((1, HEAD_DIM), F32)
    d_gain_k = jnp.zeros((1, HEAD_DIM), F32)
    for h in range(heads):
        cols = slice(h * HEAD_DIM, (h + 1) * HEAD_DIM)
        q_unit, q_rms = unit_rows(q_ref[:, cols])
        q_norm = (q_unit * gain_q).astype(BF16)
        k_unit, _ = unit_rows(jnp.concatenate([pk_ref[:, cols], k_ref[:, cols]], axis=0))
        k_norm = (k_unit * gain_k).astype(BF16)
        v_ext = jnp.concatenate([pv_ref[:, cols], v_ref[:, cols]], axis=0)
        d_out = do_ref[:, cols]
        bias = bias_blocks(table_ref[h : h + 1])
        dk = [None] * (blocks + WINDOW - 1)
        dv = [None] * (blocks + WINDOW - 1)
        d_band = [None] * WINDOW
        for p in range(blocks):
            at = slice(p * BLOCK, (p + 1) * BLOCK)
            window = slice(p * BLOCK, (p + WINDOW) * BLOCK)
            q_b, do_b, k_w, v_w = q_norm[at], d_out[at], k_norm[window], v_ext[window]
            here = [
                jnp.where(first, MASKED, b) if p + w < WINDOW - 1 else b for w, b in enumerate(bias)
            ]
            s = dot(k_w, q_b, (1, 1)) * FACTOR + jnp.concatenate(here, axis=0)
            e = jnp.exp(s - jnp.max(s, axis=0, keepdims=True))
            prob = e * (1.0 / jnp.sum(e, axis=0, keepdims=True))
            d_prob = dot(v_w, do_b, (1, 1))
            delta = jnp.sum(prob * d_prob, axis=0, keepdims=True)
            d_score = prob * (d_prob - delta)
            prob_low = prob.astype(BF16)
            d_low = d_score.astype(BF16)
            dv_w = dot(prob_low, do_b, (1, 0))
            dk_w = dot(d_low, q_b, (1, 0)) * FACTOR
            dq = dot(d_low, k_w, (0, 0)) * FACTOR
            for w in range(WINDOW):
                rng = slice(w * BLOCK, (w + 1) * BLOCK)
                dk[p + w] = dk_w[rng] if dk[p + w] is None else dk[p + w] + dk_w[rng]
                dv[p + w] = dv_w[rng] if dv[p + w] is None else dv[p + w] + dv_w[rng]
                d_band[w] = d_score[rng] if d_band[w] is None else d_band[w] + d_score[rng]
            d_gain_q = d_gain_q + jnp.sum(dq * q_unit[at], axis=0, keepdims=True)
            dq_ref[at, cols] = rows_back(dq, q_unit[at], q_rms[at], gain_q).astype(BF16)
        for b in range(blocks + WINDOW - 1):
            at = slice(b * BLOCK, (b + 1) * BLOCK)
            d_gain_k = d_gain_k + jnp.sum(dk[b] * k_unit[at], axis=0, keepdims=True)
            if b < WINDOW - 1:
                back_ref[b * BLOCK : (b + 1) * BLOCK, cols] = dk[b].astype(BF16)
                back_ref[TAIL + b * BLOCK : TAIL + (b + 1) * BLOCK, cols] = dv[b].astype(BF16)
            else:
                o = (b - WINDOW + 1) * BLOCK
                own_ref[o : o + BLOCK, cols] = dk[b]
                own_ref[rows + o : rows + o + BLOCK, cols] = dv[b]
        row = table_row(*d_band)
        pieces += [row[:, :HEAD_DIM], row[:, HEAD_DIM:]]
    pieces += [d_gain_q, d_gain_k]
    count = parts_ref.shape[1]
    pieces += [jnp.zeros((count - len(pieces), HEAD_DIM), F32)]
    parts_ref[...] = jnp.broadcast_to(jnp.concatenate(pieces, axis=0)[None], parts_ref.shape)


def final_kernel(k_ref, gains_ref, own_ref, back_ref, parts_ref, dk_ref, dv_ref, dt_ref, dg_ref):
    rows, features = k_ref.shape
    heads = features // HEAD_DIM
    sp, tp = lax.axis_size("sp"), lax.axis_size("tp")
    tail = slice(rows - TAIL, rows)
    for h in range(heads):
        cols = slice(h * HEAD_DIM, (h + 1) * HEAD_DIM)
        dk = own_ref[:rows, cols]
        dv = own_ref[rows:, cols]
        back_k = back_ref[:TAIL, cols].astype(F32)
        back_v = back_ref[TAIL:, cols].astype(F32)
        if rows > TAIL:
            zeros = jnp.zeros((rows - TAIL, HEAD_DIM), F32)
            back_k = jnp.concatenate([zeros, back_k], axis=0)
            back_v = jnp.concatenate([zeros, back_v], axis=0)
        k_unit, k_rms = unit_rows(k_ref[:, cols])
        dk_ref[:, cols] = rows_back(dk + back_k, k_unit, k_rms, gains_ref[1:2]).astype(BF16)
        dv_ref[:, cols] = (dv + back_v).astype(BF16)
    parts = parts_ref[...]
    parts = jnp.sum(parts.reshape(sp, tp, *parts.shape[1:]), axis=0)
    mine = parts[0]
    for i in range(1, tp):
        mine = jnp.where(lax.axis_index("tp") == i, parts[i], mine)
    for h in range(heads):
        row = jnp.concatenate([mine[2 * h : 2 * h + 1], mine[2 * h + 1 : 2 * h + 2]], axis=1)
        dt_ref[h : h + 1, :] = row[:, :ENTRIES]
    dg_ref[...] = jnp.sum(parts, axis=0)[2 * heads : 2 * heads + 2]


def local(queries, keys, values, gains, bias_table, d_out):
    rows, features = queries.shape
    heads = features // HEAD_DIM
    members = lax.axis_size("sp") * lax.axis_size("tp")
    count = -(-(2 * heads + 2) // 8) * 8
    prev_v = shifted(values[rows - TAIL :], 1)
    prev_k = shifted(keys[rows - TAIL :], 1)
    shape = jax.ShapeDtypeStruct
    d_queries, back, own, parts = pl.pallas_call(
        band_kernel,
        out_shape=(
            shape((rows, features), BF16),
            shape((2 * TAIL, features), BF16),
            shape((2 * rows, features), F32),
            shape((members, count, HEAD_DIM), F32),
        ),
        name="band",
    )(queries, keys, values, d_out, prev_k, prev_v, gains, bias_table.T)
    back = shifted(back, -1)
    parts = lax.all_to_all(parts, ("sp", "tp"), 0, 0)
    d_keys, d_values, d_table, d_gains = pl.pallas_call(
        final_kernel,
        out_shape=(
            shape((rows, features), BF16),
            shape((rows, features), BF16),
            shape((heads, ENTRIES), F32),
            shape((2, HEAD_DIM), F32),
        ),
        name="final",
    )(keys, gains, own, back, parts)
    return d_queries, d_keys, d_values, d_table.T, d_gains


def solution(mesh):
    in_specs = (P("sp", "tp"), P("sp", "tp"), P("sp", "tp"), P(), P(None, "tp"), P("sp", "tp"))
    out_specs = (P("sp", "tp"), P("sp", "tp"), P("sp", "tp"), P(None, "tp"), P())
    return jax.shard_map(local, mesh=mesh, in_specs=in_specs, out_specs=out_specs, check_vma=False)
```

```python
import jax
import jax.numpy as jnp
from jax import lax
from jax.experimental import pallas as pl
from jax.experimental.pallas import tpu as pltpu
from jax.sharding import PartitionSpec as P


HEAD_DIM = 128
SEG = 64
LEFT = 4
MAX_REL = 128
ENTRIES = MAX_REL + SEG
EPSILON = 1e-06
FACTOR = HEAD_DIM ** (-0.5)
TAIL = LEFT * SEG

BLOCK = 2 * SEG
WINDOW = LEFT // 2 + 1
PREV = WINDOW - 1
MASKED = -1e30

F32 = jnp.float32
BF16 = jnp.bfloat16


def dot(a, b, contract):
    return lax.dot_general(a, b, ((contract[:1], contract[1:]), ((), ())), preferred_element_type=F32)


def shifted(block, distance):
    size = lax.axis_size("sp")
    return lax.ppermute(block, "sp", [(i, (i + distance) % size) for i in range(size)])


def unit_rows(rows):
    rows = rows.astype(F32)
    inv_rms = lax.rsqrt(jnp.mean(rows * rows, axis=-1, keepdims=True) + EPSILON)
    return rows * inv_rms, inv_rms


def rows_back(d_normed, unit, inv_rms, gain):
    g = d_normed * gain
    return inv_rms * (g - unit * jnp.mean(g * unit, axis=-1, keepdims=True))


def lanes(shape):
    return lax.broadcasted_iota(jnp.int32, shape, len(shape) - 1)


def toeplitz(row):
    base = pltpu.roll(jnp.broadcast_to(row, (8, 2 * BLOCK)), 0, 1, stride=1, stride_axis=0)
    tiles = [base[:, :BLOCK]]
    for a in range(8, BLOCK, 8):
        tiles.append(pltpu.roll(base, a, 1)[:, :BLOCK])
    return jnp.concatenate(tiles, axis=0)


def diagonals(tile):
    width = 2 * BLOCK
    total = jnp.zeros((8, width), F32)
    empty = jnp.zeros((8, BLOCK), F32)
    for a in range(0, BLOCK, 8):
        part = jnp.concatenate([tile[a : a + 8], empty], axis=1)
        total = total + (pltpu.roll(part, width - a, 1) if a else part)
    out = total[:1]
    for s in range(1, 8):
        out = out + pltpu.roll(total, width - s, 1)[s : s + 1]
    return out


def bias_blocks(table):
    width = 2 * BLOCK
    last = table[:, ENTRIES - 1 :]
    lane = lanes((1, width))
    wide = jnp.concatenate([table, jnp.zeros((1, width - ENTRIES), F32)], axis=1)
    far = jnp.broadcast_to(last, (BLOCK, BLOCK))
    middle = toeplitz(jnp.where(lane < BLOCK, last, pltpu.roll(wide, width - (ENTRIES - 1), 1)))
    near = toeplitz(pltpu.roll(wide, width - (SEG - 1), 1))
    key = lax.broadcasted_iota(jnp.int32, (BLOCK, BLOCK), 0)
    query = lax.broadcasted_iota(jnp.int32, (BLOCK, BLOCK), 1)
    far = jnp.where((key < SEG) & (query >= SEG), MASKED, far)
    near = jnp.where((key >= SEG) & (query < SEG), MASKED, near)
    return [far, middle, near]


def table_row(far, middle, near):
    width = 2 * BLOCK
    lane = lanes((1, width))
    mid = diagonals(middle)
    last = jnp.sum(far) + jnp.sum(jnp.where(lane < BLOCK, mid, 0.0))
    mid = jnp.where(lane < BLOCK, 0.0, mid)
    row = pltpu.roll(diagonals(near), SEG - 1, 1) + pltpu.roll(mid, ENTRIES - 1, 1)
    return row + jnp.where(lane == ENTRIES - 1, last, 0.0)


def add(total, value):
    return value if total is None else total + value


def columns(h):
    return slice(h * HEAD_DIM, (h + 1) * HEAD_DIM)


def block_rows(b):
    return slice(b * BLOCK, (b + 1) * BLOCK)


def pair_lists(blocks):
    pairs = [(p, w) for p in range(blocks) for w in range(WINDOW)]
    return [x for x in pairs if sum(x) < PREV], [x for x in pairs if sum(x) >= PREV]


def own_kernel(
    q_hbm, k_hbm, v_hbm, do_hbm, gains_hbm, table_hbm,
    do_ref, gains_ref, qn_ref, qu_ref, qr_ref, kn_ref, ku_ref, kr_ref, bias_ref, e_ref, dp_ref, stat_ref,
    q_ref, k_ref, v_ref, table_ref, sems,
):
    moves = [(table_hbm, table_ref), (gains_hbm, gains_ref), (q_hbm, q_ref), (k_hbm, k_ref), (v_hbm, v_ref), (do_hbm, do_ref)]
    copies = [pltpu.make_async_copy(a, b, sems.at[i]) for i, (a, b) in enumerate(moves)]
    for copy in copies:
        copy.start()
    for copy in copies:
        copy.wait()
    rows, features = q_ref.shape
    blocks = rows // BLOCK
    _, own = pair_lists(blocks)
    first = lax.axis_index("sp") == 0
    for h in range(features // HEAD_DIM):
        cols = columns(h)
        q_unit, q_rms = unit_rows(q_ref[:, cols])
        k_unit, k_rms = unit_rows(k_ref[:, cols])
        q_norm = (q_unit * gains_ref[0:1]).astype(BF16)
        k_norm = (k_unit * gains_ref[1:2]).astype(BF16)
        qn_ref[:, cols], kn_ref[:, cols] = q_norm, k_norm
        qu_ref[:, cols], ku_ref[:, cols] = q_unit, k_unit
        qr_ref[:, cols] = jnp.broadcast_to(q_rms, q_unit.shape)
        kr_ref[:, cols] = jnp.broadcast_to(k_rms, k_unit.shape)
        bias = bias_blocks(table_ref[h : h + 1])
        for w in range(PREV):
            bias_ref[h, w] = jnp.where(first, MASKED, bias[w])
        for p in range(blocks):
            mine = [(i, w) for i, (pp, w) in enumerate(own) if pp == p]
            keys = slice((p + mine[0][1] - PREV) * BLOCK, (p + 1) * BLOCK)
            at = block_rows(p)
            s = dot(k_norm[keys], q_norm[at], (1, 1)) * FACTOR
            s = s + jnp.concatenate([bias[w] for _, w in mine], axis=0)
            top = jnp.max(s, axis=0, keepdims=True)
            e = jnp.exp(s - top)
            d_prob = dot(v_ref[keys, cols], do_ref[at, cols], (1, 1))
            for n, (i, _) in enumerate(mine):
                e_ref[h, i] = e[block_rows(n)]
                dp_ref[h, i] = d_prob[block_rows(n)]
            stat_ref[h, 2 * p : 2 * p + 1] = top
            stat_ref[h, 2 * p + 1 : 2 * p + 2] = jnp.sum(e, axis=0, keepdims=True)


def keys_kernel(
    pk_ref, qn_ref, do_ref, gains_ref, bias_ref, e_ref, stat_ref,
    pkn_ref, pku_ref, pp_ref, po_ref, back_ref, dv_ref,
):
    rows, features = qn_ref.shape
    blocks = rows // BLOCK
    prev, own = pair_lists(blocks)
    for h in range(features // HEAD_DIM):
        cols = columns(h)
        k_unit, _ = unit_rows(pk_ref[:, cols])
        k_norm = (k_unit * gains_ref[1:2]).astype(BF16)
        pkn_ref[:, cols], pku_ref[:, cols] = k_norm, k_unit
        dv = [None] * (blocks + PREV)
        for p in range(blocks):
            at = block_rows(p)
            top_own, sum_own = stat_ref[h, 2 * p : 2 * p + 1], stat_ref[h, 2 * p + 1 : 2 * p + 2]
            before = [(i, w) for i, (pp, w) in enumerate(prev) if pp == p]
            mine = [(i, w) for i, (pp, w) in enumerate(own) if pp == p]
            probs = {}
            if before:
                s = dot(k_norm[p * BLOCK :], qn_ref[at, cols], (1, 1)) * FACTOR
                s = s + jnp.concatenate([bias_ref[h, w] for _, w in before], axis=0)
                top = jnp.maximum(top_own, jnp.max(s, axis=0, keepdims=True))
                e = jnp.exp(s - top)
                scale = jnp.exp(top_own - top)
                inverse = 1.0 / (sum_own * scale + jnp.sum(e, axis=0, keepdims=True))
                for n, (i, w) in enumerate(before):
                    probs[w] = e[block_rows(n)] * inverse
                    pp_ref[h, i] = probs[w]
                scale = scale * inverse
            else:
                scale = 1.0 / sum_own
            for i, w in mine:
                probs[w] = e_ref[h, i] * scale
                po_ref[h, i] = probs[w]
            prob_low = jnp.concatenate([probs[w].astype(BF16) for w in range(WINDOW)], axis=0)
            dv_w = dot(prob_low, do_ref[at, cols], (1, 0))
            for w in range(WINDOW):
                dv[p + w] = add(dv[p + w], dv_w[block_rows(w)])
        for b in range(PREV):
            back_ref[block_rows(b), cols] = dv[b].astype(BF16)
        for b in range(blocks):
            dv_ref[block_rows(b), cols] = dv[PREV + b]


def values_kernel(
    pv_ref, pp_ref, po_ref, dpo_ref, do_ref, qn_ref, kn_ref, pkn_ref, qu_ref, ku_ref, pku_ref, dvb_ref,
    dq_ref, back_ref, dk_ref, parts_ref,
):
    rows, features = qn_ref.shape
    heads = features // HEAD_DIM
    blocks = rows // BLOCK
    prev, own = pair_lists(blocks)
    cells = [(h, p) for h in range(heads) for p in range(blocks)]
    d_score, d_low, pieces = {}, {}, []
    new = {}
    for h, p in cells:
        if any(pp == p for pp, _ in prev):
            new[h, p] = dot(pv_ref[p * BLOCK :, columns(h)], do_ref[block_rows(p), columns(h)], (1, 1))
    for h, p in cells:
        probs, d_probs, n = [], [], 0
        for w in range(WINDOW):
            if p + w < PREV:
                i = prev.index((p, w))
                probs.append(pp_ref[h, i])
                d_probs.append(new[h, p][block_rows(n)])
                n += 1
            else:
                i = own.index((p, w))
                probs.append(po_ref[h, i])
                d_probs.append(dpo_ref[h, i])
        delta = sum(jnp.sum(a * b, axis=0, keepdims=True) for a, b in zip(probs, d_probs))
        d_score[h, p] = [a * (b - delta) for a, b in zip(probs, d_probs)]
        d_low[h, p] = jnp.concatenate([d.astype(BF16) for d in d_score[h, p]], axis=0)
    dk = [[None] * (blocks + PREV) for _ in range(heads)]
    for h, p in cells:
        dk_w = dot(d_low[h, p], qn_ref[block_rows(p), columns(h)], (1, 0))
        for w in range(WINDOW):
            dk[h][p + w] = add(dk[h][p + w], dk_w[block_rows(w)])
    d_gain_q = jnp.zeros((1, HEAD_DIM), F32)
    d_gain_k = jnp.zeros((1, HEAD_DIM), F32)
    for h, p in cells:
        at, cols = block_rows(p), columns(h)
        k_w = [pkn_ref[block_rows(e), cols] if e < PREV else kn_ref[block_rows(e - PREV), cols] for e in range(p, p + WINDOW)]
        dq = dot(d_low[h, p], jnp.concatenate(k_w, axis=0), (0, 0)) * FACTOR
        d_gain_q = d_gain_q + jnp.sum(dq * qu_ref[at, cols], axis=0, keepdims=True)
        dq_ref[at, cols] = dq
    for h in range(heads):
        band = [sum(d_score[h, p][w] for p in range(blocks)) for w in range(WINDOW)]
        row = table_row(*band)
        pieces += [row[:, :HEAD_DIM], row[:, HEAD_DIM:]]
    for h in range(heads):
        cols = columns(h)
        for b in range(blocks + PREV):
            d_here = dk[h][b] * FACTOR
            if b < PREV:
                unit = pku_ref[block_rows(b), cols]
                back_ref[block_rows(b), cols] = d_here.astype(BF16)
                back_ref[block_rows(PREV + b), cols] = dvb_ref[block_rows(b), cols]
            else:
                unit = ku_ref[block_rows(b - PREV), cols]
                dk_ref[block_rows(b - PREV), cols] = d_here
            d_gain_k = d_gain_k + jnp.sum(d_here * unit, axis=0, keepdims=True)
    pieces += [d_gain_q, d_gain_k]
    count = parts_ref.shape[1]
    pieces += [jnp.zeros((count - len(pieces), HEAD_DIM), F32)]
    parts_ref[...] = jnp.broadcast_to(jnp.concatenate(pieces, axis=0)[None], parts_ref.shape)


def final_kernel(
    dq_ref, dk_ref, dv_ref, back_ref, qu_ref, qr_ref, ku_ref, kr_ref, gains_ref, parts_ref,
    dq_out, dk_out, dv_out, dt_ref, dg_ref,
):
    rows, features = dk_ref.shape
    heads = features // HEAD_DIM
    sp, tp = lax.axis_size("sp"), lax.axis_size("tp")
    for h in range(heads):
        cols = columns(h)
        for b in range(rows // BLOCK):
            at = block_rows(b)
            dq_out[at, cols] = rows_back(
                dq_ref[at, cols], qu_ref[at, cols], qr_ref[at, cols], gains_ref[0:1]
            ).astype(BF16)
            dk, dv = dk_ref[at, cols], dv_ref[at, cols]
            from_end = b - (rows - TAIL) // BLOCK
            if from_end >= 0:
                dk = dk + back_ref[block_rows(from_end), cols].astype(F32)
                dv = dv + back_ref[block_rows(PREV + from_end), cols].astype(F32)
            dk_out[at, cols] = rows_back(dk, ku_ref[at, cols], kr_ref[at, cols], gains_ref[1:2]).astype(BF16)
            dv_out[at, cols] = dv.astype(BF16)
    parts = parts_ref[...]
    parts = jnp.sum(parts.reshape(sp, tp, *parts.shape[1:]), axis=0)
    mine = parts[0]
    for i in range(1, tp):
        mine = jnp.where(lax.axis_index("tp") == i, parts[i], mine)
    for h in range(heads):
        row = jnp.concatenate([mine[2 * h : 2 * h + 1], mine[2 * h + 1 : 2 * h + 2]], axis=1)
        dt_ref[h : h + 1, :] = row[:, :ENTRIES]
    dg_ref[...] = jnp.sum(parts, axis=0)[2 * heads : 2 * heads + 2]


def call(kernel, name, outs, *operands, **options):
    place = jax.ShapeDtypeStruct if name == "final" else pltpu.VMEM
    return pl.pallas_call(
        kernel,
        out_shape=tuple(place(*o) for o in outs),
        **options,
        compiler_params=pltpu.CompilerParams(vmem_limit_bytes=12 << 20),
    )(*operands)


def local(queries, keys, values, gains, bias_table, d_out):
    rows, features = queries.shape
    heads = features // HEAD_DIM
    blocks = rows // BLOCK
    prev, own = (len(x) for x in pair_lists(blocks))
    members = lax.axis_size("sp") * lax.axis_size("tp")
    count = -(-(2 * heads + 2) // 8) * 8
    wide, low = ((rows, features), F32), ((rows, features), BF16)
    tail, tail_low = ((TAIL, features), F32), ((TAIL, features), BF16)
    tiles = lambda n: ((heads, n, BLOCK, BLOCK), F32)

    prev_k = shifted(keys[rows - TAIL :], 1)
    prev_v = shifted(values[rows - TAIL :], 1)
    do, g, qn, qu, qr, kn, ku, kr, bias, e_own, dp_own, stats = call(
        own_kernel, "own",
        (low, ((2, HEAD_DIM), F32), low, wide, wide, low, wide, wide, tiles(PREV), tiles(own), tiles(own),
         ((heads, 2 * blocks, BLOCK), F32)),
        *(pltpu.with_memory_space_constraint(x, pltpu.HBM) for x in (queries, keys, values, d_out, gains, bias_table.T)),
        in_specs=[pl.BlockSpec(memory_space=pltpu.HBM)] * 6,
        scratch_shapes=[pltpu.VMEM(*low)] * 3
        + [pltpu.VMEM((heads, ENTRIES), F32), pltpu.SemaphoreType.DMA((6,))],
    )
    pkn, pku, p_prev, p_own, back_v, dv_own = call(
        keys_kernel, "keys", (tail_low, tail, tiles(prev), tiles(own), tail_low, wide),
        prev_k, qn, do, g, bias, e_own, stats,
    )
    dq, back, dk_own, parts = call(
        values_kernel, "values", (wide, ((2 * TAIL, features), BF16), wide, ((members, count, HEAD_DIM), F32)),
        prev_v, p_prev, p_own, dp_own, do, qn, kn, pkn, qu, ku, pku, back_v,
    )
    back = shifted(back, -1)
    parts = lax.all_to_all(parts, ("sp", "tp"), 0, 0)
    d_queries, d_keys, d_values, d_table, d_gains = call(
        final_kernel, "final", (low, low, low, ((heads, ENTRIES), F32), ((2, HEAD_DIM), F32)),
        dq, dk_own, dv_own, back, qu, qr, ku, kr, g, parts,
    )
    return d_queries, d_keys, d_values, d_table.T, d_gains


def solution(mesh):
    in_specs = (P("sp", "tp"), P("sp", "tp"), P("sp", "tp"), P(), P(None, "tp"), P("sp", "tp"))
    out_specs = (P("sp", "tp"), P("sp", "tp"), P("sp", "tp"), P(None, "tp"), P())
    return jax.shard_map(local, mesh=mesh, in_specs=in_specs, out_specs=out_specs, check_vma=False)
```

```python
import jax
import jax.numpy as jnp
from jax import lax
from jax.experimental import pallas as pl
from jax.experimental.pallas import tpu as pltpu
from jax.sharding import PartitionSpec as P


HEAD_DIM = 128
SEG = 64
LEFT = 4
MAX_REL = 128
ENTRIES = MAX_REL + SEG
EPSILON = 1e-06
FACTOR = HEAD_DIM ** (-0.5)
TAIL = LEFT * SEG

BLOCK = 2 * SEG
WINDOW = LEFT // 2 + 1
PREV = WINDOW - 1
MASKED = -1e30

F32 = jnp.float32
BF16 = jnp.bfloat16


def dot(a, b, contract):
    return lax.dot_general(a, b, ((contract[:1], contract[1:]), ((), ())), preferred_element_type=F32)


def shifted(block, distance):
    size = lax.axis_size("sp")
    return lax.ppermute(block, "sp", [(i, (i + distance) % size) for i in range(size)])


def unit_rows(rows):
    rows = rows.astype(F32)
    inv_rms = lax.rsqrt(jnp.mean(rows * rows, axis=-1, keepdims=True) + EPSILON)
    return rows * inv_rms, inv_rms


def rows_back(d_normed, unit, inv_rms, gain):
    g = d_normed * gain
    return inv_rms * (g - unit * jnp.mean(g * unit, axis=-1, keepdims=True))


def lanes(shape):
    return lax.broadcasted_iota(jnp.int32, shape, len(shape) - 1)


def toeplitz(row):
    base = pltpu.roll(jnp.broadcast_to(row, (8, 2 * BLOCK)), 0, 1, stride=1, stride_axis=0)
    tiles = [base[:, :BLOCK]]
    for a in range(8, BLOCK, 8):
        tiles.append(pltpu.roll(base, a, 1)[:, :BLOCK])
    return jnp.concatenate(tiles, axis=0)


def diagonals(tile):
    width = 2 * BLOCK
    total = jnp.zeros((8, width), F32)
    empty = jnp.zeros((8, BLOCK), F32)
    for a in range(0, BLOCK, 8):
        part = jnp.concatenate([tile[a : a + 8], empty], axis=1)
        total = total + (pltpu.roll(part, width - a, 1) if a else part)
    out = total[:1]
    for s in range(1, 8):
        out = out + pltpu.roll(total, width - s, 1)[s : s + 1]
    return out


def bias_blocks(table):
    width = 2 * BLOCK
    last = table[:, ENTRIES - 1 :]
    lane = lanes((1, width))
    wide = jnp.concatenate([table, jnp.zeros((1, width - ENTRIES), F32)], axis=1)
    far = jnp.broadcast_to(last, (BLOCK, BLOCK))
    middle = toeplitz(jnp.where(lane < BLOCK, last, pltpu.roll(wide, width - (ENTRIES - 1), 1)))
    near = toeplitz(pltpu.roll(wide, width - (SEG - 1), 1))
    key = lax.broadcasted_iota(jnp.int32, (BLOCK, BLOCK), 0)
    query = lax.broadcasted_iota(jnp.int32, (BLOCK, BLOCK), 1)
    far = jnp.where((key < SEG) & (query >= SEG), MASKED, far)
    near = jnp.where((key >= SEG) & (query < SEG), MASKED, near)
    return [far, middle, near]


def table_row(far, middle, near):
    width = 2 * BLOCK
    lane = lanes((1, width))
    mid = diagonals(middle)
    last = jnp.sum(far) + jnp.sum(jnp.where(lane < BLOCK, mid, 0.0))
    mid = jnp.where(lane < BLOCK, 0.0, mid)
    row = pltpu.roll(diagonals(near), SEG - 1, 1) + pltpu.roll(mid, ENTRIES - 1, 1)
    return row + jnp.where(lane == ENTRIES - 1, last, 0.0)


def add(total, value):
    return value if total is None else total + value


def columns(h):
    return slice(h * HEAD_DIM, (h + 1) * HEAD_DIM)


def block_rows(b):
    return slice(b * BLOCK, (b + 1) * BLOCK)


def pair_lists(blocks):
    pairs = [(p, w) for p in range(blocks) for w in range(WINDOW)]
    return [x for x in pairs if sum(x) < PREV], [x for x in pairs if sum(x) >= PREV]


def own_kernel(
    q_hbm, k_hbm, v_hbm, do_hbm, gains_hbm, table_hbm,
    do_ref, gains_ref, qn_ref, qu_ref, qr_ref, kn_ref, ku_ref, kr_ref, bias_ref, e_ref, dp_ref, stat_ref,
    q_ref, k_ref, v_ref, table_ref, sems,
):
    moves = [(table_hbm, table_ref), (gains_hbm, gains_ref), (q_hbm, q_ref), (k_hbm, k_ref), (v_hbm, v_ref), (do_hbm, do_ref)]
    copies = [pltpu.make_async_copy(a, b, sems.at[i]) for i, (a, b) in enumerate(moves)]
    for copy in copies:
        copy.start()
    for copy in copies:
        copy.wait()
    rows, features = q_ref.shape
    blocks = rows // BLOCK
    _, own = pair_lists(blocks)
    first = lax.axis_index("sp") == 0
    for h in range(features // HEAD_DIM):
        cols = columns(h)
        q_unit, q_rms = unit_rows(q_ref[:, cols])
        k_unit, k_rms = unit_rows(k_ref[:, cols])
        q_norm = (q_unit * gains_ref[0:1]).astype(BF16)
        k_norm = (k_unit * gains_ref[1:2]).astype(BF16)
        qn_ref[:, cols], kn_ref[:, cols] = q_norm, k_norm
        qu_ref[:, cols], ku_ref[:, cols] = q_unit, k_unit
        qr_ref[:, cols] = jnp.broadcast_to(q_rms, q_unit.shape)
        kr_ref[:, cols] = jnp.broadcast_to(k_rms, k_unit.shape)
        bias = bias_blocks(table_ref[h : h + 1])
        for w in range(PREV):
            bias_ref[h, w] = jnp.where(first, MASKED, bias[w])
        for p in range(blocks):
            mine = [(i, w) for i, (pp, w) in enumerate(own) if pp == p]
            keys = slice((p + mine[0][1] - PREV) * BLOCK, (p + 1) * BLOCK)
            at = block_rows(p)
            s = dot(k_norm[keys], q_norm[at], (1, 1)) * FACTOR
            s = s + jnp.concatenate([bias[w] for _, w in mine], axis=0)
            top = jnp.max(s, axis=0, keepdims=True)
            e = jnp.exp(s - top)
            d_prob = dot(v_ref[keys, cols], do_ref[at, cols], (1, 1))
            for n, (i, _) in enumerate(mine):
                e_ref[h, i] = e[block_rows(n)]
                dp_ref[h, i] = d_prob[block_rows(n)]
            stat_ref[h, 2 * p : 2 * p + 1] = top
            stat_ref[h, 2 * p + 1 : 2 * p + 2] = jnp.sum(e, axis=0, keepdims=True)


def keys_kernel(
    pk_ref, qn_ref, do_ref, gains_ref, bias_ref, e_ref, stat_ref,
    pkn_ref, pku_ref, pp_ref, po_ref, back_ref, dv_ref,
):
    rows, features = qn_ref.shape
    blocks = rows // BLOCK
    prev, own = pair_lists(blocks)
    heads = features // HEAD_DIM
    cells = [(h, p) for h in range(heads) for p in range(blocks)]
    joined = [(h, p) for h, p in cells if p < PREV]
    k_norm, s, scale = {}, {}, {}
    for h in range(heads):
        k_unit, _ = unit_rows(pk_ref[:, columns(h)])
        k_norm[h] = (k_unit * gains_ref[1:2]).astype(BF16)
        pkn_ref[:, columns(h)], pku_ref[:, columns(h)] = k_norm[h], k_unit
    for h, p in joined:
        s[h, p] = dot(k_norm[h][p * BLOCK :], qn_ref[block_rows(p), columns(h)], (1, 1))
    prob = {}
    for h, p in cells:
        top_own, sum_own = stat_ref[h, 2 * p : 2 * p + 1], stat_ref[h, 2 * p + 1 : 2 * p + 2]
        scale = 1.0
        total = sum_own
        if (h, p) in joined:
            bias = jnp.concatenate([bias_ref[h, w] for w in range(PREV - p)], axis=0)
            scores = s[h, p] * FACTOR + bias
            top = jnp.maximum(top_own, jnp.max(scores, axis=0, keepdims=True))
            e = jnp.exp(scores - top)
            scale = jnp.exp(top_own - top)
            total = sum_own * scale + jnp.sum(e, axis=0, keepdims=True)
        inverse = 1.0 / total
        scale = scale * inverse
        parts = []
        for w in range(WINDOW):
            if p + w < PREV:
                i = prev.index((p, w))
                parts.append(e[block_rows(w)] * inverse)
                pp_ref[h, i] = parts[w]
            else:
                i = own.index((p, w))
                parts.append(e_ref[h, i] * scale)
                po_ref[h, i] = parts[w]
        prob[h, p] = jnp.concatenate([x.astype(BF16) for x in parts], axis=0)
    dv = [[None] * (blocks + PREV) for _ in range(heads)]
    for h, p in cells:
        dv_w = dot(prob[h, p], do_ref[block_rows(p), columns(h)], (1, 0))
        for w in range(WINDOW):
            dv[h][p + w] = add(dv[h][p + w], dv_w[block_rows(w)])
    for h in range(heads):
        for b in range(PREV):
            back_ref[block_rows(b), columns(h)] = dv[h][b].astype(BF16)
        for b in range(blocks):
            dv_ref[block_rows(b), columns(h)] = dv[h][PREV + b]


def values_kernel(
    pv_ref, pp_ref, po_ref, dpo_ref, do_ref, qn_ref, kn_ref, pkn_ref, qu_ref, ku_ref, pku_ref, dvb_ref,
    dq_ref, back_ref, dk_ref, parts_ref,
):
    rows, features = qn_ref.shape
    heads = features // HEAD_DIM
    blocks = rows // BLOCK
    prev, own = pair_lists(blocks)
    cells = [(h, p) for h in range(heads) for p in range(blocks)]
    d_score, d_low, pieces = {}, {}, []
    new = {}
    for h, p in cells:
        if any(pp == p for pp, _ in prev):
            new[h, p] = dot(pv_ref[p * BLOCK :, columns(h)], do_ref[block_rows(p), columns(h)], (1, 1))
    for h, p in cells:
        probs, d_probs, n = [], [], 0
        for w in range(WINDOW):
            if p + w < PREV:
                i = prev.index((p, w))
                probs.append(pp_ref[h, i])
                d_probs.append(new[h, p][block_rows(n)])
                n += 1
            else:
                i = own.index((p, w))
                probs.append(po_ref[h, i])
                d_probs.append(dpo_ref[h, i])
        delta = sum(jnp.sum(a * b, axis=0, keepdims=True) for a, b in zip(probs, d_probs))
        d_score[h, p] = [a * (b - delta) for a, b in zip(probs, d_probs)]
        d_low[h, p] = jnp.concatenate([d.astype(BF16) for d in d_score[h, p]], axis=0)
    dk = [[None] * (blocks + PREV) for _ in range(heads)]
    for h, p in cells:
        dk_w = dot(d_low[h, p], qn_ref[block_rows(p), columns(h)], (1, 0))
        for w in range(WINDOW):
            dk[h][p + w] = add(dk[h][p + w], dk_w[block_rows(w)])
    d_gain_q = jnp.zeros((1, HEAD_DIM), F32)
    d_gain_k = jnp.zeros((1, HEAD_DIM), F32)
    for h, p in cells:
        at, cols = block_rows(p), columns(h)
        k_w = [pkn_ref[block_rows(e), cols] if e < PREV else kn_ref[block_rows(e - PREV), cols] for e in range(p, p + WINDOW)]
        dq = dot(d_low[h, p], jnp.concatenate(k_w, axis=0), (0, 0)) * FACTOR
        d_gain_q = d_gain_q + jnp.sum(dq * qu_ref[at, cols], axis=0, keepdims=True)
        dq_ref[at, cols] = dq
    for h in range(heads):
        band = [sum(d_score[h, p][w] for p in range(blocks)) for w in range(WINDOW)]
        row = table_row(*band)
        pieces.append(row[:, :ENTRIES])
    for h in range(heads):
        cols = columns(h)
        for b in range(blocks + PREV):
            d_here = dk[h][b] * FACTOR
            if b < PREV:
                unit = pku_ref[block_rows(b), cols]
                back_ref[block_rows(b), cols] = d_here.astype(BF16)
                back_ref[block_rows(PREV + b), cols] = dvb_ref[block_rows(b), cols]
            else:
                unit = ku_ref[block_rows(b - PREV), cols]
                dk_ref[block_rows(b - PREV), cols] = d_here
            d_gain_k = d_gain_k + jnp.sum(d_here * unit, axis=0, keepdims=True)
    width = parts_ref.shape[2]
    gap = width - heads * ENTRIES - 2 * HEAD_DIM
    pieces += ([jnp.zeros((1, gap), F32)] if gap else []) + [d_gain_q, d_gain_k]
    flat = jnp.concatenate(pieces, axis=1)
    for c in range(0, width, HEAD_DIM):
        at = slice(c, c + HEAD_DIM)
        parts_ref[:, :, at] = jnp.broadcast_to(flat[None, :, at], (parts_ref.shape[0], 1, HEAD_DIM))


def final_kernel(
    dq_ref, dk_ref, dv_ref, back_ref, qu_ref, qr_ref, ku_ref, kr_ref, gains_ref, parts_ref,
    dq_out, dk_out, dv_out, dt_ref, dg_ref,
):
    rows, features = dk_ref.shape
    heads = features // HEAD_DIM
    tp = lax.axis_size("tp")
    for h in range(heads):
        cols = columns(h)
        for b in range(rows // BLOCK):
            at = block_rows(b)
            dq_out[at, cols] = rows_back(
                dq_ref[at, cols], qu_ref[at, cols], qr_ref[at, cols], gains_ref[0:1]
            ).astype(BF16)
            dk, dv = dk_ref[at, cols], dv_ref[at, cols]
            from_end = b - (rows - TAIL) // BLOCK
            if from_end >= 0:
                dk = dk + back_ref[block_rows(from_end), cols].astype(F32)
                dv = dv + back_ref[block_rows(PREV + from_end), cols].astype(F32)
            dk_out[at, cols] = rows_back(dk, ku_ref[at, cols], kr_ref[at, cols], gains_ref[1:2]).astype(BF16)
            dv_out[at, cols] = dv.astype(BF16)
    members = parts_ref.shape[0]
    width = parts_ref.shape[2]
    sums = [parts_ref[i] for i in range(tp)]
    for n in range(tp, members):
        sums[n % tp] = sums[n % tp] + parts_ref[n]
    mine, total = sums[0], sums[0]
    for i in range(1, tp):
        mine = jnp.where(lax.axis_index("tp") == i, sums[i], mine)
        total = total + sums[i]
    for h in range(heads):
        dt_ref[h : h + 1, :] = mine[:, h * ENTRIES : (h + 1) * ENTRIES]
    dg_ref[0:1] = total[:, width - 2 * HEAD_DIM : width - HEAD_DIM]
    dg_ref[1:2] = total[:, width - HEAD_DIM :]


def call(kernel, name, outs, *operands, **options):
    place = jax.ShapeDtypeStruct if name == "final" else pltpu.VMEM
    return pl.pallas_call(
        kernel,
        out_shape=tuple(place(*o) for o in outs),
        **options,
        compiler_params=pltpu.CompilerParams(vmem_limit_bytes=12 << 20),
    )(*operands)


def local(queries, keys, values, gains, bias_table, d_out):
    rows, features = queries.shape
    heads = features // HEAD_DIM
    blocks = rows // BLOCK
    prev, own = (len(x) for x in pair_lists(blocks))
    members = lax.axis_size("sp") * lax.axis_size("tp")
    width = (-(-heads * ENTRIES // HEAD_DIM) + 2) * HEAD_DIM
    wide, low = ((rows, features), F32), ((rows, features), BF16)
    tail, tail_low = ((TAIL, features), F32), ((TAIL, features), BF16)
    tiles = lambda n: ((heads, n, BLOCK, BLOCK), F32)

    prev_k = shifted(keys[rows - TAIL :], 1)
    prev_v = shifted(values[rows - TAIL :], 1)
    do, g, qn, qu, qr, kn, ku, kr, bias, e_own, dp_own, stats = call(
        own_kernel, "own",
        (low, ((2, HEAD_DIM), F32), low, wide, wide, low, wide, wide, tiles(PREV), tiles(own), tiles(own),
         ((heads, 2 * blocks, BLOCK), F32)),
        *(pltpu.with_memory_space_constraint(x, pltpu.HBM) for x in (queries, keys, values, d_out, gains, bias_table.T)),
        in_specs=[pl.BlockSpec(memory_space=pltpu.HBM)] * 6,
        scratch_shapes=[pltpu.VMEM(*low)] * 3
        + [pltpu.VMEM((heads, ENTRIES), F32), pltpu.SemaphoreType.DMA((6,))],
    )
    pkn, pku, p_prev, p_own, back_v, dv_own = call(
        keys_kernel, "keys", (tail_low, tail, tiles(prev), tiles(own), tail_low, wide),
        prev_k, qn, do, g, bias, e_own, stats,
    )
    dq, back, dk_own, parts = call(
        values_kernel, "values", (wide, ((2 * TAIL, features), BF16), wide, ((members, 1, width), F32)),
        prev_v, p_prev, p_own, dp_own, do, qn, kn, pkn, qu, ku, pku, back_v,
    )
    back = shifted(back, -1)
    parts = lax.all_to_all(parts, ("sp", "tp"), 0, 0)
    d_queries, d_keys, d_values, d_table, d_gains = call(
        final_kernel, "final", (low, low, low, ((heads, ENTRIES), F32), ((2, HEAD_DIM), F32)),
        dq, dk_own, dv_own, back, qu, qr, ku, kr, g, parts,
    )
    return d_queries, d_keys, d_values, d_table.T, d_gains


def solution(mesh):
    in_specs = (P("sp", "tp"), P("sp", "tp"), P("sp", "tp"), P(), P(None, "tp"), P("sp", "tp"))
    out_specs = (P("sp", "tp"), P("sp", "tp"), P("sp", "tp"), P(None, "tp"), P())
    return jax.shard_map(local, mesh=mesh, in_specs=in_specs, out_specs=out_specs, check_vma=False)
```

```python
import jax
import jax.numpy as jnp
from jax import lax
from jax.experimental import pallas as pl
from jax.experimental.pallas import tpu as pltpu
from jax.sharding import PartitionSpec as P


HEAD_DIM = 128
SEG = 64
LEFT = 4
MAX_REL = 128
ENTRIES = MAX_REL + SEG
EPSILON = 1e-06
FACTOR = HEAD_DIM ** (-0.5)
TAIL = LEFT * SEG

BLOCK = 2 * SEG
WINDOW = LEFT // 2 + 1
PREV = WINDOW - 1
MASKED = -1e30

F32 = jnp.float32
BF16 = jnp.bfloat16


def dot(a, b, contract):
    return lax.dot_general(a, b, ((contract[:1], contract[1:]), ((), ())), preferred_element_type=F32)


def shifted(block, distance):
    size = lax.axis_size("sp")
    return lax.ppermute(block, "sp", [(i, (i + distance) % size) for i in range(size)])


def unit_rows(rows):
    rows = rows.astype(F32)
    inv_rms = lax.rsqrt(jnp.mean(rows * rows, axis=-1, keepdims=True) + EPSILON)
    return rows * inv_rms, inv_rms


def rows_back(d_normed, unit, inv_rms, gain):
    g = d_normed * gain
    return inv_rms * (g - unit * jnp.mean(g * unit, axis=-1, keepdims=True))


def lanes(shape):
    return lax.broadcasted_iota(jnp.int32, shape, len(shape) - 1)


def toeplitz(row):
    base = pltpu.roll(jnp.broadcast_to(row, (8, 2 * BLOCK)), 0, 1, stride=1, stride_axis=0)
    tiles = [base[:, :BLOCK]]
    for a in range(8, BLOCK, 8):
        tiles.append(pltpu.roll(base, a, 1)[:, :BLOCK])
    return jnp.concatenate(tiles, axis=0)


def diagonals(tile):
    width = 2 * BLOCK
    total = jnp.zeros((8, width), F32)
    empty = jnp.zeros((8, BLOCK), F32)
    for a in range(0, BLOCK, 8):
        part = jnp.concatenate([tile[a : a + 8], empty], axis=1)
        total = total + (pltpu.roll(part, width - a, 1) if a else part)
    out = total[:1]
    for s in range(1, 8):
        out = out + pltpu.roll(total, width - s, 1)[s : s + 1]
    return out


def bias_blocks(table):
    width = 2 * BLOCK
    last = table[:, ENTRIES - 1 :]
    lane = lanes((1, width))
    wide = jnp.concatenate([table, jnp.zeros((1, width - ENTRIES), F32)], axis=1)
    far = jnp.broadcast_to(last, (BLOCK, BLOCK))
    middle = toeplitz(jnp.where(lane < BLOCK, last, pltpu.roll(wide, width - (ENTRIES - 1), 1)))
    near = toeplitz(pltpu.roll(wide, width - (SEG - 1), 1))
    key = lax.broadcasted_iota(jnp.int32, (BLOCK, BLOCK), 0)
    query = lax.broadcasted_iota(jnp.int32, (BLOCK, BLOCK), 1)
    far = jnp.where((key < SEG) & (query >= SEG), MASKED, far)
    near = jnp.where((key >= SEG) & (query < SEG), MASKED, near)
    return [far, middle, near]


def table_row(far, middle, near):
    width = 2 * BLOCK
    lane = lanes((1, width))
    mid = diagonals(middle)
    last = jnp.sum(far) + jnp.sum(jnp.where(lane < BLOCK, mid, 0.0))
    mid = jnp.where(lane < BLOCK, 0.0, mid)
    row = pltpu.roll(diagonals(near), SEG - 1, 1) + pltpu.roll(mid, ENTRIES - 1, 1)
    return row + jnp.where(lane == ENTRIES - 1, last, 0.0)


def add(total, value):
    return value if total is None else total + value


def columns(h):
    return slice(h * HEAD_DIM, (h + 1) * HEAD_DIM)


def block_rows(b):
    return slice(b * BLOCK, (b + 1) * BLOCK)


def pair_lists(blocks):
    pairs = [(p, w) for p in range(blocks) for w in range(WINDOW)]
    return [x for x in pairs if sum(x) < PREV], [x for x in pairs if sum(x) >= PREV]


def own_kernel(
    q_hbm, k_hbm, v_hbm, do_hbm, gains_hbm, table_hbm,
    do_ref, gains_ref, qn_ref, qu_ref, qr_ref, kn_ref, ku_ref, kr_ref, bias_ref, e_ref, dp_ref, stat_ref,
    q_ref, k_ref, v_ref, table_ref, sems,
):
    moves = [(table_hbm, table_ref), (gains_hbm, gains_ref), (q_hbm, q_ref), (k_hbm, k_ref), (v_hbm, v_ref), (do_hbm, do_ref)]
    copies = [pltpu.make_async_copy(a, b, sems.at[i]) for i, (a, b) in enumerate(moves)]
    for copy in copies:
        copy.start()
    for copy in copies:
        copy.wait()
    rows, features = q_ref.shape
    blocks = rows // BLOCK
    _, own = pair_lists(blocks)
    first = lax.axis_index("sp") == 0
    for h in range(features // HEAD_DIM):
        cols = columns(h)
        q_unit, q_rms = unit_rows(q_ref[:, cols])
        k_unit, k_rms = unit_rows(k_ref[:, cols])
        q_norm = (q_unit * gains_ref[0:1]).astype(BF16)
        k_norm = (k_unit * gains_ref[1:2]).astype(BF16)
        qn_ref[:, cols], kn_ref[:, cols] = q_norm, k_norm
        qu_ref[:, cols], ku_ref[:, cols] = q_unit, k_unit
        qr_ref[:, cols] = jnp.broadcast_to(q_rms, q_unit.shape)
        kr_ref[:, cols] = jnp.broadcast_to(k_rms, k_unit.shape)
        bias = bias_blocks(table_ref[h : h + 1])
        for w in range(PREV):
            bias_ref[h, w] = jnp.where(first, MASKED, bias[w])
        for p in range(blocks):
            mine = [(i, w) for i, (pp, w) in enumerate(own) if pp == p]
            keys = slice((p + mine[0][1] - PREV) * BLOCK, (p + 1) * BLOCK)
            at = block_rows(p)
            s = dot(k_norm[keys], q_norm[at], (1, 1)) * FACTOR
            s = s + jnp.concatenate([bias[w] for _, w in mine], axis=0)
            top = jnp.max(s, axis=0, keepdims=True)
            e = jnp.exp(s - top)
            d_prob = dot(v_ref[keys, cols], do_ref[at, cols], (1, 1))
            for n, (i, _) in enumerate(mine):
                e_ref[h, i] = e[block_rows(n)]
                dp_ref[h, i] = d_prob[block_rows(n)]
            stat_ref[h, 2 * p : 2 * p + 1] = top
            stat_ref[h, 2 * p + 1 : 2 * p + 2] = jnp.sum(e, axis=0, keepdims=True)


def keys_kernel(
    pk_ref, qn_ref, do_ref, gains_ref, bias_ref, e_ref, stat_ref,
    pkn_ref, pku_ref, pp_ref, po_ref, back_ref, dv_ref,
):
    rows, features = qn_ref.shape
    blocks = rows // BLOCK
    prev, own = pair_lists(blocks)
    heads = features // HEAD_DIM
    cells = [(h, p) for h in range(heads) for p in range(blocks)]
    joined = [(h, p) for h, p in cells if p < PREV]
    k_norm, s, scale = {}, {}, {}
    for h in range(heads):
        k_unit, _ = unit_rows(pk_ref[:, columns(h)])
        k_norm[h] = (k_unit * gains_ref[1:2]).astype(BF16)
        pkn_ref[:, columns(h)], pku_ref[:, columns(h)] = k_norm[h], k_unit
    for h, p in joined:
        s[h, p] = dot(k_norm[h][p * BLOCK :], qn_ref[block_rows(p), columns(h)], (1, 1))
    prob = {}
    for h, p in cells:
        top_own, sum_own = stat_ref[h, 2 * p : 2 * p + 1], stat_ref[h, 2 * p + 1 : 2 * p + 2]
        scale = 1.0
        total = sum_own
        if (h, p) in joined:
            bias = jnp.concatenate([bias_ref[h, w] for w in range(PREV - p)], axis=0)
            scores = s[h, p] * FACTOR + bias
            top = jnp.maximum(top_own, jnp.max(scores, axis=0, keepdims=True))
            e = jnp.exp(scores - top)
            scale = jnp.exp(top_own - top)
            total = sum_own * scale + jnp.sum(e, axis=0, keepdims=True)
        inverse = 1.0 / total
        scale = scale * inverse
        parts = []
        for w in range(WINDOW):
            if p + w < PREV:
                i = prev.index((p, w))
                parts.append(e[block_rows(w)] * inverse)
                pp_ref[h, i] = parts[w]
            else:
                i = own.index((p, w))
                parts.append(e_ref[h, i] * scale)
                po_ref[h, i] = parts[w]
        prob[h, p] = jnp.concatenate([x.astype(BF16) for x in parts], axis=0)
    dv = [[None] * (blocks + PREV) for _ in range(heads)]
    for h, p in cells:
        dv_w = dot(prob[h, p], do_ref[block_rows(p), columns(h)], (1, 0))
        for w in range(WINDOW):
            dv[h][p + w] = add(dv[h][p + w], dv_w[block_rows(w)])
    for h in range(heads):
        for b in range(PREV):
            back_ref[block_rows(PREV + b), columns(h)] = dv[h][b].astype(BF16)
        for b in range(blocks):
            dv_ref[block_rows(b), columns(h)] = dv[h][PREV + b]


def values_kernel(
    pv_ref, pp_ref, po_ref, dpo_ref, do_ref, qn_ref, kn_ref, pkn_ref, qu_ref, ku_ref, pku_ref, _,
    dq_ref, back_ref, dk_ref, parts_ref,
):
    rows, features = qn_ref.shape
    heads = features // HEAD_DIM
    blocks = rows // BLOCK
    prev, own = pair_lists(blocks)
    cells = [(h, p) for h in range(heads) for p in range(blocks)]
    d_score, d_low, pieces = {}, {}, []
    new = {}
    for h, p in cells:
        if any(pp == p for pp, _ in prev):
            new[h, p] = dot(pv_ref[p * BLOCK :, columns(h)], do_ref[block_rows(p), columns(h)], (1, 1))
    for h, p in cells:
        probs, d_probs, n = [], [], 0
        for w in range(WINDOW):
            if p + w < PREV:
                i = prev.index((p, w))
                probs.append(pp_ref[h, i])
                d_probs.append(new[h, p][block_rows(n)])
                n += 1
            else:
                i = own.index((p, w))
                probs.append(po_ref[h, i])
                d_probs.append(dpo_ref[h, i])
        delta = sum(jnp.sum(a * b, axis=0, keepdims=True) for a, b in zip(probs, d_probs))
        d_score[h, p] = [a * (b - delta) for a, b in zip(probs, d_probs)]
        d_low[h, p] = jnp.concatenate([d.astype(BF16) for d in d_score[h, p]], axis=0)
    dk = [[None] * (blocks + PREV) for _ in range(heads)]
    for h, p in cells:
        dk_w = dot(d_low[h, p], qn_ref[block_rows(p), columns(h)], (1, 0))
        for w in range(WINDOW):
            dk[h][p + w] = add(dk[h][p + w], dk_w[block_rows(w)])
    d_gain_q = jnp.zeros((1, HEAD_DIM), F32)
    d_gain_k = jnp.zeros((1, HEAD_DIM), F32)
    for h, p in cells:
        at, cols = block_rows(p), columns(h)
        k_w = [pkn_ref[block_rows(e), cols] if e < PREV else kn_ref[block_rows(e - PREV), cols] for e in range(p, p + WINDOW)]
        dq = dot(d_low[h, p], jnp.concatenate(k_w, axis=0), (0, 0)) * FACTOR
        d_gain_q = d_gain_q + jnp.sum(dq * qu_ref[at, cols], axis=0, keepdims=True)
        dq_ref[at, cols] = dq
    for h in range(heads):
        band = [sum(d_score[h, p][w] for p in range(blocks)) for w in range(WINDOW)]
        row = table_row(*band)
        pieces.append(row[:, :ENTRIES])
    for h in range(heads):
        cols = columns(h)
        for b in range(blocks + PREV):
            d_here = dk[h][b] * FACTOR
            if b < PREV:
                unit = pku_ref[block_rows(b), cols]
                back_ref[block_rows(b), cols] = d_here.astype(BF16)
            else:
                unit = ku_ref[block_rows(b - PREV), cols]
                dk_ref[block_rows(b - PREV), cols] = d_here
            d_gain_k = d_gain_k + jnp.sum(d_here * unit, axis=0, keepdims=True)
    gap = -heads * ENTRIES % HEAD_DIM
    pieces += ([jnp.zeros((1, gap), F32)] if gap else []) + [d_gain_q, d_gain_k]
    flat = jnp.concatenate(pieces, axis=1)
    lines = [flat[:, c : c + HEAD_DIM] for c in range(0, flat.shape[1], HEAD_DIM)]
    once = jnp.concatenate(lines * 8, axis=0)
    for r in range(0, parts_ref.shape[0], once.shape[0]):
        parts_ref[r : r + once.shape[0]] = once


def final_kernel(
    dq_ref, dk_ref, dv_ref, back_ref, qu_ref, qr_ref, ku_ref, kr_ref, gains_ref, parts_ref,
    dq_out, dk_out, dv_out, dt_ref, dg_ref,
):
    rows, features = dk_ref.shape
    heads = features // HEAD_DIM
    tp = lax.axis_size("tp")
    for h in range(heads):
        cols = columns(h)
        for b in range(rows // BLOCK):
            at = block_rows(b)
            dq_out[at, cols] = rows_back(
                dq_ref[at, cols], qu_ref[at, cols], qr_ref[at, cols], gains_ref[0:1]
            ).astype(BF16)
            dk, dv = dk_ref[at, cols], dv_ref[at, cols]
            from_end = b - (rows - TAIL) // BLOCK
            if from_end >= 0:
                dk = dk + back_ref[block_rows(from_end), cols].astype(F32)
                dv = dv + back_ref[block_rows(PREV + from_end), cols].astype(F32)
            dk_out[at, cols] = rows_back(dk, ku_ref[at, cols], kr_ref[at, cols], gains_ref[1:2]).astype(BF16)
            dv_out[at, cols] = dv.astype(BF16)
    members = parts_ref.shape[0]
    width = parts_ref.shape[2]
    sums = [parts_ref[i] for i in range(tp)]
    for n in range(tp, members):
        sums[n % tp] = sums[n % tp] + parts_ref[n]
    mine, total = sums[0], sums[0]
    for i in range(1, tp):
        mine = jnp.where(lax.axis_index("tp") == i, sums[i], mine)
        total = total + sums[i]
    for h in range(heads):
        dt_ref[h : h + 1, :] = mine[:, h * ENTRIES : (h + 1) * ENTRIES]
    dg_ref[0:1] = total[:, width - 2 * HEAD_DIM : width - HEAD_DIM]
    dg_ref[1:2] = total[:, width - HEAD_DIM :]


def call(kernel, name, outs, *operands, **options):
    place = jax.ShapeDtypeStruct if name == "final" else pltpu.VMEM
    return pl.pallas_call(
        kernel,
        out_shape=tuple(place(*o) for o in outs),
        **options,
        compiler_params=pltpu.CompilerParams(vmem_limit_bytes=12 << 20),
    )(*operands)


def local(queries, keys, values, gains, bias_table, d_out):
    rows, features = queries.shape
    heads = features // HEAD_DIM
    blocks = rows // BLOCK
    prev, own = (len(x) for x in pair_lists(blocks))
    members = lax.axis_size("sp") * lax.axis_size("tp")
    width = (-(-heads * ENTRIES // HEAD_DIM) + 2) * HEAD_DIM
    wide, low = ((rows, features), F32), ((rows, features), BF16)
    tail, tail_low = ((TAIL, features), F32), ((TAIL, features), BF16)
    tiles = lambda n: ((heads, n, BLOCK, BLOCK), F32)

    prev_k = shifted(keys[rows - TAIL :], 1)
    prev_v = shifted(values[rows - TAIL :], 1)
    do, g, qn, qu, qr, kn, ku, kr, bias, e_own, dp_own, stats = call(
        own_kernel, "own",
        (low, ((2, HEAD_DIM), F32), low, wide, wide, low, wide, wide, tiles(PREV), tiles(own), tiles(own),
         ((heads, 2 * blocks, BLOCK), F32)),
        *(pltpu.with_memory_space_constraint(x, pltpu.HBM) for x in (queries, keys, values, d_out, gains, bias_table.T)),
        in_specs=[pl.BlockSpec(memory_space=pltpu.HBM)] * 6,
        scratch_shapes=[pltpu.VMEM(*low)] * 3
        + [pltpu.VMEM((heads, ENTRIES), F32), pltpu.SemaphoreType.DMA((6,))],
    )
    pkn, pku, p_prev, p_own, back_v, dv_own = call(
        keys_kernel, "keys", (tail_low, tail, tiles(prev), tiles(own), ((2 * TAIL, features), BF16), wide),
        prev_k, qn, do, g, bias, e_own, stats,
    )
    dq, back, dk_own, parts = call(
        values_kernel, "values", (wide, ((2 * TAIL, features), BF16), wide, ((members * width // HEAD_DIM, HEAD_DIM), F32)),
        prev_v, p_prev, p_own, dp_own, do, qn, kn, pkn, qu, ku, pku, back_v, input_output_aliases={11: 1},
    )
    back = shifted(back, -1)
    parts = lax.all_to_all(parts.reshape(members, 1, width), ("sp", "tp"), 0, 0)
    d_queries, d_keys, d_values, d_table, d_gains = call(
        final_kernel, "final", (low, low, low, ((heads, ENTRIES), F32), ((2, HEAD_DIM), F32)),
        dq, dk_own, dv_own, back, qu, qr, ku, kr, g, parts,
    )
    return d_queries, d_keys, d_values, d_table.T, d_gains


def solution(mesh):
    in_specs = (P("sp", "tp"), P("sp", "tp"), P("sp", "tp"), P(), P(None, "tp"), P("sp", "tp"))
    out_specs = (P("sp", "tp"), P("sp", "tp"), P("sp", "tp"), P(None, "tp"), P())
    return jax.shard_map(local, mesh=mesh, in_specs=in_specs, out_specs=out_specs, check_vma=False)
```

```python
import jax
import jax.numpy as jnp
from jax import lax
from jax.experimental import pallas as pl
from jax.experimental.pallas import tpu as pltpu
from jax.sharding import PartitionSpec as P


HEAD_DIM = 128
SEG = 64
LEFT = 4
MAX_REL = 128
ENTRIES = MAX_REL + SEG
EPSILON = 1e-06
FACTOR = HEAD_DIM ** (-0.5)
TAIL = LEFT * SEG

BLOCK = 2 * SEG
WINDOW = LEFT // 2 + 1
PREV = WINDOW - 1
MASKED = -1e30

F32 = jnp.float32
BF16 = jnp.bfloat16


def dot(a, b, contract):
    return lax.dot_general(a, b, ((contract[:1], contract[1:]), ((), ())), preferred_element_type=F32)


def shifted(block, distance):
    size = lax.axis_size("sp")
    return lax.ppermute(block, "sp", [(i, (i + distance) % size) for i in range(size)])


def unit_rows(rows):
    rows = rows.astype(F32)
    inv_rms = lax.rsqrt(jnp.mean(rows * rows, axis=-1, keepdims=True) + EPSILON)
    return rows * inv_rms, inv_rms


def rows_back(d_normed, unit, inv_rms, gain):
    g = d_normed * gain
    return inv_rms * (g - unit * jnp.mean(g * unit, axis=-1, keepdims=True))


def lanes(shape):
    return lax.broadcasted_iota(jnp.int32, shape, len(shape) - 1)


def toeplitz(row):
    base = pltpu.roll(jnp.broadcast_to(row, (8, 2 * BLOCK)), 0, 1, stride=1, stride_axis=0)
    tiles = [base[:, :BLOCK]]
    for a in range(8, BLOCK, 8):
        tiles.append(pltpu.roll(base, a, 1)[:, :BLOCK])
    return jnp.concatenate(tiles, axis=0)


def diagonals(tile):
    width = 2 * BLOCK
    total = jnp.zeros((8, width), F32)
    empty = jnp.zeros((8, BLOCK), F32)
    for a in range(0, BLOCK, 8):
        part = jnp.concatenate([tile[a : a + 8], empty], axis=1)
        total = total + (pltpu.roll(part, width - a, 1) if a else part)
    out = total[:1]
    for s in range(1, 8):
        out = out + pltpu.roll(total, width - s, 1)[s : s + 1]
    return out


def bias_blocks(table):
    width = 2 * BLOCK
    last = table[:, ENTRIES - 1 :]
    lane = lanes((1, width))
    wide = jnp.concatenate([table, jnp.zeros((1, width - ENTRIES), F32)], axis=1)
    far = jnp.broadcast_to(last, (BLOCK, BLOCK))
    middle = toeplitz(jnp.where(lane < BLOCK, last, pltpu.roll(wide, width - (ENTRIES - 1), 1)))
    near = toeplitz(pltpu.roll(wide, width - (SEG - 1), 1))
    key = lax.broadcasted_iota(jnp.int32, (BLOCK, BLOCK), 0)
    query = lax.broadcasted_iota(jnp.int32, (BLOCK, BLOCK), 1)
    far = jnp.where((key < SEG) & (query >= SEG), MASKED, far)
    near = jnp.where((key >= SEG) & (query < SEG), MASKED, near)
    return [far, middle, near]


def table_row(far, middle, near):
    width = 2 * BLOCK
    lane = lanes((1, width))
    mid = diagonals(middle)
    last = jnp.sum(far) + jnp.sum(jnp.where(lane < BLOCK, mid, 0.0))
    mid = jnp.where(lane < BLOCK, 0.0, mid)
    row = pltpu.roll(diagonals(near), SEG - 1, 1) + pltpu.roll(mid, ENTRIES - 1, 1)
    return row + jnp.where(lane == ENTRIES - 1, last, 0.0)


def add(total, value):
    return value if total is None else total + value


def columns(h):
    return slice(h * HEAD_DIM, (h + 1) * HEAD_DIM)


def block_rows(b):
    return slice(b * BLOCK, (b + 1) * BLOCK)


def pair_lists(blocks):
    pairs = [(p, w) for p in range(blocks) for w in range(WINDOW)]
    return [x for x in pairs if sum(x) < PREV], [x for x in pairs if sum(x) >= PREV]


def own_kernel(
    q_hbm, k_hbm, v_hbm, do_hbm, gains_hbm, table_hbm,
    do_ref, gains_ref, qn_ref, qu_ref, qr_ref, kn_ref, ku_ref, kr_ref, bias_ref, e_ref, dp_ref, stat_ref,
    q_ref, k_ref, v_ref, table_ref, sems,
):
    moves = [(table_hbm, table_ref), (gains_hbm, gains_ref), (q_hbm, q_ref), (k_hbm, k_ref), (v_hbm, v_ref), (do_hbm, do_ref)]
    copies = [pltpu.make_async_copy(a, b, sems.at[i]) for i, (a, b) in enumerate(moves)]
    for copy in copies:
        copy.start()
    for copy in copies:
        copy.wait()
    rows, features = q_ref.shape
    blocks = rows // BLOCK
    _, own = pair_lists(blocks)
    first = lax.axis_index("sp") == 0
    for h in range(features // HEAD_DIM):
        cols = columns(h)
        q_unit, q_rms = unit_rows(q_ref[:, cols])
        k_unit, k_rms = unit_rows(k_ref[:, cols])
        q_norm = (q_unit * gains_ref[0:1]).astype(BF16)
        k_norm = (k_unit * gains_ref[1:2]).astype(BF16)
        qn_ref[:, cols], kn_ref[:, cols] = q_norm, k_norm
        qu_ref[:, cols], ku_ref[:, cols] = q_unit, k_unit
        qr_ref[:, cols] = jnp.broadcast_to(q_rms, q_unit.shape)
        kr_ref[:, cols] = jnp.broadcast_to(k_rms, k_unit.shape)
        bias = bias_blocks(table_ref[h : h + 1])
        for w in range(PREV):
            bias_ref[h, w] = jnp.where(first, MASKED, bias[w])
        for p in range(blocks):
            mine = [(i, w) for i, (pp, w) in enumerate(own) if pp == p]
            keys = slice((p + mine[0][1] - PREV) * BLOCK, (p + 1) * BLOCK)
            at = block_rows(p)
            s = dot(k_norm[keys], q_norm[at], (1, 1)) * FACTOR
            s = s + jnp.concatenate([bias[w] for _, w in mine], axis=0)
            top = jnp.max(s, axis=0, keepdims=True)
            e = jnp.exp(s - top)
            d_prob = dot(v_ref[keys, cols], do_ref[at, cols], (1, 1))
            for n, (i, _) in enumerate(mine):
                e_ref[h, i] = e[block_rows(n)]
                dp_ref[h, i] = d_prob[block_rows(n)]
            stat_ref[h, 2 * p : 2 * p + 1] = top
            stat_ref[h, 2 * p + 1 : 2 * p + 2] = jnp.sum(e, axis=0, keepdims=True)


def keys_kernel(
    pk_ref, qn_ref, do_ref, gains_ref, bias_ref, e_ref, stat_ref,
    pkn_ref, pku_ref, pp_ref, po_ref, back_ref, dv_ref,
):
    rows, features = qn_ref.shape
    blocks = rows // BLOCK
    prev, own = pair_lists(blocks)
    heads = features // HEAD_DIM
    cells = [(h, p) for h in range(heads) for p in range(blocks)]
    joined = [(h, p) for h, p in cells if p < PREV]
    k_norm, s, scale = {}, {}, {}
    for h in range(heads):
        k_unit, _ = unit_rows(pk_ref[:, columns(h)])
        k_norm[h] = (k_unit * gains_ref[1:2]).astype(BF16)
        pkn_ref[:, columns(h)], pku_ref[:, columns(h)] = k_norm[h], k_unit
    for h, p in joined:
        s[h, p] = dot(k_norm[h][p * BLOCK :], qn_ref[block_rows(p), columns(h)], (1, 1))
    prob = {}
    for h, p in cells:
        top_own, sum_own = stat_ref[h, 2 * p : 2 * p + 1], stat_ref[h, 2 * p + 1 : 2 * p + 2]
        scale = 1.0
        total = sum_own
        if (h, p) in joined:
            bias = jnp.concatenate([bias_ref[h, w] for w in range(PREV - p)], axis=0)
            scores = s[h, p] * FACTOR + bias
            top = jnp.maximum(top_own, jnp.max(scores, axis=0, keepdims=True))
            e = jnp.exp(scores - top)
            scale = jnp.exp(top_own - top)
            total = sum_own * scale + jnp.sum(e, axis=0, keepdims=True)
        inverse = 1.0 / total
        scale = scale * inverse
        parts = []
        for w in range(WINDOW):
            if p + w < PREV:
                i = prev.index((p, w))
                parts.append(e[block_rows(w)] * inverse)
                pp_ref[h, i] = parts[w]
            else:
                i = own.index((p, w))
                parts.append(e_ref[h, i] * scale)
                po_ref[h, i] = parts[w]
        prob[h, p] = jnp.concatenate([x.astype(BF16) for x in parts], axis=0)
    dv = [[None] * (blocks + PREV) for _ in range(heads)]
    for h, p in cells:
        dv_w = dot(prob[h, p], do_ref[block_rows(p), columns(h)], (1, 0))
        for w in range(WINDOW):
            dv[h][p + w] = add(dv[h][p + w], dv_w[block_rows(w)])
    for h in range(heads):
        for b in range(PREV):
            back_ref[block_rows(PREV + b), columns(h)] = dv[h][b].astype(BF16)
        for b in range(blocks):
            dv_ref[block_rows(b), columns(h)] = dv[h][PREV + b]


def values_kernel(
    pv_ref, pp_ref, po_ref, dpo_ref, do_ref, qn_ref, kn_ref, pkn_ref, qu_ref, ku_ref, pku_ref, _,
    dq_ref, back_ref, dk_ref, parts_ref,
):
    rows, features = qn_ref.shape
    heads = features // HEAD_DIM
    blocks = rows // BLOCK
    prev, own = pair_lists(blocks)
    cells = [(h, p) for h in range(heads) for p in range(blocks)]
    d_score, d_low, pieces = {}, {}, []
    new = {}
    for h, p in cells:
        if any(pp == p for pp, _ in prev):
            new[h, p] = dot(pv_ref[p * BLOCK :, columns(h)], do_ref[block_rows(p), columns(h)], (1, 1))
    for h, p in cells:
        probs, d_probs, n = [], [], 0
        for w in range(WINDOW):
            if p + w < PREV:
                i = prev.index((p, w))
                probs.append(pp_ref[h, i])
                d_probs.append(new[h, p][block_rows(n)])
                n += 1
            else:
                i = own.index((p, w))
                probs.append(po_ref[h, i])
                d_probs.append(dpo_ref[h, i])
        delta = sum(jnp.sum(a * b, axis=0, keepdims=True) for a, b in zip(probs, d_probs))
        d_score[h, p] = [a * (b - delta) for a, b in zip(probs, d_probs)]
        d_low[h, p] = jnp.concatenate([d.astype(BF16) for d in d_score[h, p]], axis=0)
    dk = [[None] * (blocks + PREV) for _ in range(heads)]
    for h, p in cells:
        dk_w = dot(d_low[h, p], qn_ref[block_rows(p), columns(h)], (1, 0))
        for w in range(WINDOW):
            dk[h][p + w] = add(dk[h][p + w], dk_w[block_rows(w)])
    d_gain_q = jnp.zeros((1, HEAD_DIM), F32)
    d_gain_k = jnp.zeros((1, HEAD_DIM), F32)
    for h, p in cells:
        at, cols = block_rows(p), columns(h)
        k_w = [pkn_ref[block_rows(e), cols] if e < PREV else kn_ref[block_rows(e - PREV), cols] for e in range(p, p + WINDOW)]
        dq = dot(d_low[h, p], jnp.concatenate(k_w, axis=0), (0, 0)) * FACTOR
        d_gain_q = d_gain_q + jnp.sum(dq * qu_ref[at, cols], axis=0, keepdims=True)
        dq_ref[at, cols] = dq
    for h in range(heads):
        band = [sum(d_score[h, p][w] for p in range(blocks)) for w in range(WINDOW)]
        row = table_row(*band)
        pieces.append(row[:, :ENTRIES])
    for h in range(heads):
        cols = columns(h)
        for b in range(blocks + PREV):
            d_here = dk[h][b] * FACTOR
            if b < PREV:
                unit = pku_ref[block_rows(b), cols]
                back_ref[block_rows(b), cols] = d_here.astype(BF16)
            else:
                unit = ku_ref[block_rows(b - PREV), cols]
                dk_ref[block_rows(b - PREV), cols] = d_here
            d_gain_k = d_gain_k + jnp.sum(d_here * unit, axis=0, keepdims=True)
    gap = -heads * ENTRIES % HEAD_DIM
    pieces += ([jnp.zeros((1, gap), F32)] if gap else []) + [d_gain_q, d_gain_k]
    flat = jnp.concatenate(pieces, axis=1)
    lines = [flat[:, c : c + HEAD_DIM] for c in range(0, flat.shape[1], HEAD_DIM)]
    once = jnp.concatenate(lines * 8, axis=0)
    for r in range(0, parts_ref.shape[0], once.shape[0]):
        parts_ref[r : r + once.shape[0]] = once


def final_kernel(
    dq_ref, dk_ref, dv_ref, back_ref, qu_ref, qr_ref, ku_ref, kr_ref, gains_ref, parts_ref,
    dq_out, dk_out, dv_out, dt_ref, dg_ref,
):
    rows, features = dk_ref.shape
    heads = features // HEAD_DIM
    tp = lax.axis_size("tp")
    for h in range(heads):
        cols = columns(h)
        for b in range(rows // BLOCK):
            at = block_rows(b)
            dq_out[at, cols] = rows_back(
                dq_ref[at, cols], qu_ref[at, cols], qr_ref[at, cols], gains_ref[0:1]
            ).astype(BF16)
            dk, dv = dk_ref[at, cols], dv_ref[at, cols]
            from_end = b - (rows - TAIL) // BLOCK
            if from_end >= 0:
                dk = dk + back_ref[block_rows(from_end), cols].astype(F32)
                dv = dv + back_ref[block_rows(PREV + from_end), cols].astype(F32)
            dk_out[at, cols] = rows_back(dk, ku_ref[at, cols], kr_ref[at, cols], gains_ref[1:2]).astype(BF16)
            dv_out[at, cols] = dv.astype(BF16)
    members = parts_ref.shape[0]
    width = parts_ref.shape[2]
    each = members // tp
    sums = [parts_ref[i * each] for i in range(tp)]
    for n in range(1, each):
        sums = [x + parts_ref[i * each + n] for i, x in enumerate(sums)]
    mine, total = sums[0], sums[0]
    for i in range(1, tp):
        mine = jnp.where(lax.axis_index("tp") == i, sums[i], mine)
        total = total + sums[i]
    for h in range(heads):
        dt_ref[h : h + 1, :] = mine[:, h * ENTRIES : (h + 1) * ENTRIES]
    dg_ref[0:1] = total[:, width - 2 * HEAD_DIM : width - HEAD_DIM]
    dg_ref[1:2] = total[:, width - HEAD_DIM :]


def call(kernel, name, outs, *operands, **options):
    place = jax.ShapeDtypeStruct if name == "final" else pltpu.VMEM
    return pl.pallas_call(
        kernel,
        out_shape=tuple(place(*o) for o in outs),
        **options,
        compiler_params=pltpu.CompilerParams(vmem_limit_bytes=12 << 20),
    )(*operands)


def local(queries, keys, values, gains, bias_table, d_out):
    rows, features = queries.shape
    heads = features // HEAD_DIM
    blocks = rows // BLOCK
    prev, own = (len(x) for x in pair_lists(blocks))
    members = lax.axis_size("sp") * lax.axis_size("tp")
    width = (-(-heads * ENTRIES // HEAD_DIM) + 2) * HEAD_DIM
    wide, low = ((rows, features), F32), ((rows, features), BF16)
    tail, tail_low = ((TAIL, features), F32), ((TAIL, features), BF16)
    tiles = lambda n: ((heads, n, BLOCK, BLOCK), F32)

    prev_k = shifted(keys[rows - TAIL :], 1)
    prev_v = shifted(values[rows - TAIL :], 1)
    do, g, qn, qu, qr, kn, ku, kr, bias, e_own, dp_own, stats = call(
        own_kernel, "own",
        (low, ((2, HEAD_DIM), F32), low, wide, wide, low, wide, wide, tiles(PREV), tiles(own), tiles(own),
         ((heads, 2 * blocks, BLOCK), F32)),
        *(pltpu.with_memory_space_constraint(x, pltpu.HBM) for x in (queries, keys, values, d_out, gains, bias_table.T)),
        in_specs=[pl.BlockSpec(memory_space=pltpu.HBM)] * 6,
        scratch_shapes=[pltpu.VMEM(*low)] * 3
        + [pltpu.VMEM((heads, ENTRIES), F32), pltpu.SemaphoreType.DMA((6,))],
    )
    pkn, pku, p_prev, p_own, back_v, dv_own = call(
        keys_kernel, "keys", (tail_low, tail, tiles(prev), tiles(own), ((2 * TAIL, features), BF16), wide),
        prev_k, qn, do, g, bias, e_own, stats,
    )
    dq, back, dk_own, parts = call(
        values_kernel, "values", (wide, ((2 * TAIL, features), BF16), wide, ((members * width // HEAD_DIM, HEAD_DIM), F32)),
        prev_v, p_prev, p_own, dp_own, do, qn, kn, pkn, qu, ku, pku, back_v, input_output_aliases={11: 1},
    )
    back = shifted(back, -1)
    parts = lax.all_to_all(parts.reshape(members, 1, width), ("tp", "sp"), 0, 0)
    d_queries, d_keys, d_values, d_table, d_gains = call(
        final_kernel, "final", (low, low, low, ((heads, ENTRIES), F32), ((2, HEAD_DIM), F32)),
        dq, dk_own, dv_own, back, qu, qr, ku, kr, g, parts,
    )
    return d_queries, d_keys, d_values, d_table.T, d_gains


def solution(mesh):
    in_specs = (P("sp", "tp"), P("sp", "tp"), P("sp", "tp"), P(), P(None, "tp"), P("sp", "tp"))
    out_specs = (P("sp", "tp"), P("sp", "tp"), P("sp", "tp"), P(None, "tp"), P())
    return jax.shard_map(local, mesh=mesh, in_specs=in_specs, out_specs=out_specs, check_vma=False)
```

```python
import jax
import jax.numpy as jnp
from jax import lax
from jax.experimental import pallas as pl
from jax.experimental.pallas import tpu as pltpu
from jax.sharding import PartitionSpec as P


HEAD_DIM = 128
SEG = 64
LEFT = 4
MAX_REL = 128
ENTRIES = MAX_REL + SEG
EPSILON = 1e-06
FACTOR = HEAD_DIM ** (-0.5)
TAIL = LEFT * SEG

BLOCK = 2 * SEG
WINDOW = LEFT // 2 + 1
PREV = WINDOW - 1
MASKED = -1e30

F32 = jnp.float32
BF16 = jnp.bfloat16


def dot(a, b, contract):
    return lax.dot_general(a, b, ((contract[:1], contract[1:]), ((), ())), preferred_element_type=F32)


def shifted(block, distance):
    size = lax.axis_size("sp")
    return lax.ppermute(block, "sp", [(i, (i + distance) % size) for i in range(size)])


def unit_rows(rows):
    rows = rows.astype(F32)
    inv_rms = lax.rsqrt(jnp.mean(rows * rows, axis=-1, keepdims=True) + EPSILON)
    return rows * inv_rms, inv_rms


def rows_back(d_normed, unit, inv_rms, gain):
    g = d_normed * gain
    return inv_rms * (g - unit * jnp.mean(g * unit, axis=-1, keepdims=True))


def lanes(shape):
    return lax.broadcasted_iota(jnp.int32, shape, len(shape) - 1)


def toeplitz(row):
    base = pltpu.roll(jnp.broadcast_to(row, (8, 2 * BLOCK)), 0, 1, stride=1, stride_axis=0)
    tiles = [base[:, :BLOCK]]
    for a in range(8, BLOCK, 8):
        tiles.append(pltpu.roll(base, a, 1)[:, :BLOCK])
    return jnp.concatenate(tiles, axis=0)


def diagonals(tile):
    width = 2 * BLOCK
    total = jnp.zeros((8, width), F32)
    empty = jnp.zeros((8, BLOCK), F32)
    for a in range(0, BLOCK, 8):
        part = jnp.concatenate([tile[a : a + 8], empty], axis=1)
        total = total + (pltpu.roll(part, width - a, 1) if a else part)
    out = total[:1]
    for s in range(1, 8):
        out = out + pltpu.roll(total, width - s, 1)[s : s + 1]
    return out


def bias_blocks(table):
    width = 2 * BLOCK
    last = table[:, ENTRIES - 1 :]
    lane = lanes((1, width))
    wide = jnp.concatenate([table, jnp.zeros((1, width - ENTRIES), F32)], axis=1)
    far = jnp.broadcast_to(last, (BLOCK, BLOCK))
    middle = toeplitz(jnp.where(lane < BLOCK, last, pltpu.roll(wide, width - (ENTRIES - 1), 1)))
    near = toeplitz(pltpu.roll(wide, width - (SEG - 1), 1))
    key = lax.broadcasted_iota(jnp.int32, (BLOCK, BLOCK), 0)
    query = lax.broadcasted_iota(jnp.int32, (BLOCK, BLOCK), 1)
    far = jnp.where((key < SEG) & (query >= SEG), MASKED, far)
    near = jnp.where((key >= SEG) & (query < SEG), MASKED, near)
    return [far, middle, near]


def table_row(far, middle, near):
    width = 2 * BLOCK
    lane = lanes((1, width))
    mid = diagonals(middle)
    last = jnp.sum(far) + jnp.sum(jnp.where(lane < BLOCK, mid, 0.0))
    mid = jnp.where(lane < BLOCK, 0.0, mid)
    row = pltpu.roll(diagonals(near), SEG - 1, 1) + pltpu.roll(mid, ENTRIES - 1, 1)
    return row + jnp.where(lane == ENTRIES - 1, last, 0.0)


def add(total, value):
    return value if total is None else total + value


def columns(h):
    return slice(h * HEAD_DIM, (h + 1) * HEAD_DIM)


def block_rows(b):
    return slice(b * BLOCK, (b + 1) * BLOCK)


def pair_lists(blocks):
    pairs = [(p, w) for p in range(blocks) for w in range(WINDOW)]
    return [x for x in pairs if sum(x) < PREV], [x for x in pairs if sum(x) >= PREV]


def own_kernel(
    q_hbm, k_hbm, v_hbm, do_hbm, gains_hbm, table_hbm,
    do_ref, gains_ref, qn_ref, qu_ref, qr_ref, kn_ref, ku_ref, kr_ref, bias_ref, e_ref, dp_ref, stat_ref,
    q_ref, k_ref, v_ref, table_ref, sems,
):
    moves = [(table_hbm, table_ref), (gains_hbm, gains_ref), (q_hbm, q_ref), (k_hbm, k_ref), (v_hbm, v_ref), (do_hbm, do_ref)]
    copies = [pltpu.make_async_copy(a, b, sems.at[i]) for i, (a, b) in enumerate(moves)]
    for copy in copies:
        copy.start()
    for copy in copies:
        copy.wait()
    rows, features = q_ref.shape
    blocks = rows // BLOCK
    _, own = pair_lists(blocks)
    first = lax.axis_index("sp") == 0
    for h in range(features // HEAD_DIM):
        cols = columns(h)
        q_unit, q_rms = unit_rows(q_ref[:, cols])
        k_unit, k_rms = unit_rows(k_ref[:, cols])
        q_norm = (q_unit * gains_ref[0:1]).astype(BF16)
        k_norm = (k_unit * gains_ref[1:2]).astype(BF16)
        qn_ref[:, cols], kn_ref[:, cols] = q_norm, k_norm
        qu_ref[:, cols], ku_ref[:, cols] = q_unit, k_unit
        qr_ref[:, cols] = jnp.broadcast_to(q_rms, q_unit.shape)
        kr_ref[:, cols] = jnp.broadcast_to(k_rms, k_unit.shape)
        bias = bias_blocks(table_ref[h : h + 1])
        for w in range(PREV):
            bias_ref[h, w] = jnp.where(first, MASKED, bias[w])
        for p in range(blocks):
            mine = [(i, w) for i, (pp, w) in enumerate(own) if pp == p]
            keys = slice((p + mine[0][1] - PREV) * BLOCK, (p + 1) * BLOCK)
            at = block_rows(p)
            s = dot(k_norm[keys], q_norm[at], (1, 1)) * FACTOR
            s = s + jnp.concatenate([bias[w] for _, w in mine], axis=0)
            top = jnp.max(s, axis=0, keepdims=True)
            e = jnp.exp(s - top)
            d_prob = dot(v_ref[keys, cols], do_ref[at, cols], (1, 1))
            for n, (i, _) in enumerate(mine):
                e_ref[h, i] = e[block_rows(n)]
                dp_ref[h, i] = d_prob[block_rows(n)]
            stat_ref[h, 2 * p : 2 * p + 1] = top
            stat_ref[h, 2 * p + 1 : 2 * p + 2] = jnp.sum(e, axis=0, keepdims=True)


def keys_kernel(
    pk_ref, qn_ref, do_ref, gains_ref, bias_ref, e_ref, stat_ref,
    pkn_ref, pku_ref, pp_ref, po_ref, back_ref, dv_ref,
):
    rows, features = qn_ref.shape
    blocks = rows // BLOCK
    prev, own = pair_lists(blocks)
    heads = features // HEAD_DIM
    cells = [(h, p) for h in range(heads) for p in range(blocks)]
    joined = [(h, p) for h, p in cells if p < PREV]
    k_norm, s, scale = {}, {}, {}
    for h in range(heads):
        k_unit, _ = unit_rows(pk_ref[:, columns(h)])
        k_norm[h] = (k_unit * gains_ref[1:2]).astype(BF16)
        pkn_ref[:, columns(h)], pku_ref[:, columns(h)] = k_norm[h], k_unit
    for h, p in joined:
        s[h, p] = dot(k_norm[h][p * BLOCK :], qn_ref[block_rows(p), columns(h)], (1, 1))
    prob = {}
    for h, p in cells:
        top_own, sum_own = stat_ref[h, 2 * p : 2 * p + 1], stat_ref[h, 2 * p + 1 : 2 * p + 2]
        scale = 1.0
        total = sum_own
        if (h, p) in joined:
            bias = jnp.concatenate([bias_ref[h, w] for w in range(PREV - p)], axis=0)
            scores = s[h, p] * FACTOR + bias
            top = jnp.maximum(top_own, jnp.max(scores, axis=0, keepdims=True))
            e = jnp.exp(scores - top)
            scale = jnp.exp(top_own - top)
            total = sum_own * scale + jnp.sum(e, axis=0, keepdims=True)
        inverse = 1.0 / total
        scale = scale * inverse
        parts = []
        for w in range(WINDOW):
            if p + w < PREV:
                i = prev.index((p, w))
                parts.append(e[block_rows(w)] * inverse)
                pp_ref[h, i] = parts[w]
            else:
                i = own.index((p, w))
                parts.append(e_ref[h, i] * scale)
                po_ref[h, i] = parts[w]
        prob[h, p] = jnp.concatenate([x.astype(BF16) for x in parts], axis=0)
    dv = [[None] * (blocks + PREV) for _ in range(heads)]
    for h, p in cells:
        dv_w = dot(prob[h, p], do_ref[block_rows(p), columns(h)], (1, 0))
        for w in range(WINDOW):
            dv[h][p + w] = add(dv[h][p + w], dv_w[block_rows(w)])
    for h in range(heads):
        for b in range(PREV):
            back_ref[block_rows(PREV + b), columns(h)] = dv[h][b].astype(BF16)
        for b in range(blocks):
            dv_ref[block_rows(b), columns(h)] = dv[h][PREV + b]


def values_kernel(
    pv_ref, pp_ref, po_ref, dpo_ref, do_ref, qn_ref, kn_ref, pkn_ref, qu_ref, ku_ref, pku_ref, _,
    dq_ref, back_ref, dk_ref, parts_ref,
):
    rows, features = qn_ref.shape
    heads = features // HEAD_DIM
    blocks = rows // BLOCK
    prev, own = pair_lists(blocks)
    cells = [(h, p) for h in range(heads) for p in range(blocks)]
    d_score, d_low, pieces = {}, {}, []
    new = {}
    for h, p in cells:
        if any(pp == p for pp, _ in prev):
            new[h, p] = dot(pv_ref[p * BLOCK :, columns(h)], do_ref[block_rows(p), columns(h)], (1, 1))
    for h, p in cells:
        probs, d_probs, n = [], [], 0
        for w in range(WINDOW):
            if p + w < PREV:
                i = prev.index((p, w))
                probs.append(pp_ref[h, i])
                d_probs.append(new[h, p][block_rows(n)])
                n += 1
            else:
                i = own.index((p, w))
                probs.append(po_ref[h, i])
                d_probs.append(dpo_ref[h, i])
        delta = sum(jnp.sum(a * b, axis=0, keepdims=True) for a, b in zip(probs, d_probs))
        d_score[h, p] = [a * (b - delta) for a, b in zip(probs, d_probs)]
        d_low[h, p] = jnp.concatenate([d.astype(BF16) for d in d_score[h, p]], axis=0)
    dk = [[None] * (blocks + PREV) for _ in range(heads)]
    for h, p in cells:
        dk_w = dot(d_low[h, p], qn_ref[block_rows(p), columns(h)], (1, 0))
        for w in range(WINDOW):
            dk[h][p + w] = add(dk[h][p + w], dk_w[block_rows(w)])
    d_gain_q = jnp.zeros((1, HEAD_DIM), F32)
    d_gain_k = jnp.zeros((1, HEAD_DIM), F32)
    for h, p in cells:
        at, cols = block_rows(p), columns(h)
        k_w = [pkn_ref[block_rows(e), cols] if e < PREV else kn_ref[block_rows(e - PREV), cols] for e in range(p, p + WINDOW)]
        dq = dot(d_low[h, p], jnp.concatenate(k_w, axis=0), (0, 0)) * FACTOR
        d_gain_q = d_gain_q + jnp.sum(dq * qu_ref[at, cols], axis=0, keepdims=True)
        dq_ref[at, cols] = dq
    for h in range(heads):
        band = [sum(d_score[h, p][w] for p in range(blocks)) for w in range(WINDOW)]
        row = table_row(*band)
        pieces.append(row[:, :ENTRIES])
    for h in range(heads):
        cols = columns(h)
        for b in range(blocks + PREV):
            d_here = dk[h][b] * FACTOR
            if b < PREV:
                unit = pku_ref[block_rows(b), cols]
                back_ref[block_rows(b), cols] = d_here.astype(BF16)
            else:
                unit = ku_ref[block_rows(b - PREV), cols]
                dk_ref[block_rows(b - PREV), cols] = d_here
            d_gain_k = d_gain_k + jnp.sum(d_here * unit, axis=0, keepdims=True)
    gap = -heads * ENTRIES % HEAD_DIM
    pieces += ([jnp.zeros((1, gap), F32)] if gap else []) + [d_gain_q, d_gain_k]
    flat = jnp.concatenate(pieces, axis=1)
    lines = [flat[:, c : c + HEAD_DIM] for c in range(0, flat.shape[1], HEAD_DIM)]
    once = jnp.concatenate(lines * 8, axis=0)
    for r in range(0, parts_ref.shape[0], once.shape[0]):
        parts_ref[r : r + once.shape[0]] = once


def final_kernel(
    dq_ref, dk_ref, dv_ref, back_ref, qu_ref, qr_ref, ku_ref, kr_ref, gains_ref, parts_ref,
    dq_out, dk_out, dv_out, dt_ref, dg_ref,
):
    rows, features = dk_ref.shape
    heads = features // HEAD_DIM
    tp = lax.axis_size("tp")
    for h in range(heads):
        cols = columns(h)
        for b in range(rows // BLOCK):
            at = block_rows(b)
            dq_out[at, cols] = rows_back(
                dq_ref[at, cols], qu_ref[at, cols], qr_ref[at, cols], gains_ref[0:1]
            ).astype(BF16)
            dk, dv = dk_ref[at, cols], dv_ref[at, cols]
            from_end = b - (rows - TAIL) // BLOCK
            if from_end >= 0:
                dk = dk + back_ref[block_rows(from_end), cols].astype(F32)
                dv = dv + back_ref[block_rows(PREV + from_end), cols].astype(F32)
            dk_out[at, cols] = rows_back(dk, ku_ref[at, cols], kr_ref[at, cols], gains_ref[1:2]).astype(BF16)
            dv_out[at, cols] = dv.astype(BF16)
    lines = -(-heads * ENTRIES // HEAD_DIM) + 2
    width = lines * HEAD_DIM
    each, group = parts_ref.shape[0] // tp, 8 * lines
    sums = []
    for i in range(tp):
        fold = parts_ref[i * each : i * each + group]
        for r in range(group, each, group):
            fold = fold + parts_ref[i * each + r : i * each + r + group]
        rows_of = [sum(fold[n : n + 1] for n in range(c, group, lines)) for c in range(lines)]
        sums.append(jnp.concatenate(rows_of, axis=1))
    mine, total = sums[0], sums[0]
    for i in range(1, tp):
        mine = jnp.where(lax.axis_index("tp") == i, sums[i], mine)
        total = total + sums[i]
    for h in range(heads):
        dt_ref[h : h + 1, :] = mine[:, h * ENTRIES : (h + 1) * ENTRIES]
    dg_ref[0:1] = total[:, width - 2 * HEAD_DIM : width - HEAD_DIM]
    dg_ref[1:2] = total[:, width - HEAD_DIM :]


def call(kernel, name, outs, *operands, **options):
    place = jax.ShapeDtypeStruct if name == "final" else pltpu.VMEM
    return pl.pallas_call(
        kernel,
        out_shape=tuple(place(*o) for o in outs),
        **options,
        compiler_params=pltpu.CompilerParams(vmem_limit_bytes=12 << 20),
    )(*operands)


def local(queries, keys, values, gains, bias_table, d_out):
    rows, features = queries.shape
    heads = features // HEAD_DIM
    blocks = rows // BLOCK
    prev, own = (len(x) for x in pair_lists(blocks))
    members = lax.axis_size("sp") * lax.axis_size("tp")
    width = (-(-heads * ENTRIES // HEAD_DIM) + 2) * HEAD_DIM
    wide, low = ((rows, features), F32), ((rows, features), BF16)
    tail, tail_low = ((TAIL, features), F32), ((TAIL, features), BF16)
    tiles = lambda n: ((heads, n, BLOCK, BLOCK), F32)

    prev_k = shifted(keys[rows - TAIL :], 1)
    prev_v = shifted(values[rows - TAIL :], 1)
    do, g, qn, qu, qr, kn, ku, kr, bias, e_own, dp_own, stats = call(
        own_kernel, "own",
        (low, ((2, HEAD_DIM), F32), low, wide, wide, low, wide, wide, tiles(PREV), tiles(own), tiles(own),
         ((heads, 2 * blocks, BLOCK), F32)),
        *(pltpu.with_memory_space_constraint(x, pltpu.HBM) for x in (queries, keys, values, d_out, gains, bias_table.T)),
        in_specs=[pl.BlockSpec(memory_space=pltpu.HBM)] * 6,
        scratch_shapes=[pltpu.VMEM(*low)] * 3
        + [pltpu.VMEM((heads, ENTRIES), F32), pltpu.SemaphoreType.DMA((6,))],
    )
    pkn, pku, p_prev, p_own, back_v, dv_own = call(
        keys_kernel, "keys", (tail_low, tail, tiles(prev), tiles(own), ((2 * TAIL, features), BF16), wide),
        prev_k, qn, do, g, bias, e_own, stats,
    )
    dq, back, dk_own, parts = call(
        values_kernel, "values", (wide, ((2 * TAIL, features), BF16), wide, ((members * width // HEAD_DIM, HEAD_DIM), F32)),
        prev_v, p_prev, p_own, dp_own, do, qn, kn, pkn, qu, ku, pku, back_v, input_output_aliases={11: 1},
    )
    back = shifted(back, -1)
    parts = lax.all_to_all(parts.reshape(members, 1, width), ("tp", "sp"), 0, 0)
    parts = parts.reshape(members * width // HEAD_DIM, HEAD_DIM)
    d_queries, d_keys, d_values, d_table, d_gains = call(
        final_kernel, "final", (low, low, low, ((heads, ENTRIES), F32), ((2, HEAD_DIM), F32)),
        dq, dk_own, dv_own, back, qu, qr, ku, kr, g, parts,
    )
    return d_queries, d_keys, d_values, d_table.T, d_gains


def solution(mesh):
    in_specs = (P("sp", "tp"), P("sp", "tp"), P("sp", "tp"), P(), P(None, "tp"), P("sp", "tp"))
    out_specs = (P("sp", "tp"), P("sp", "tp"), P("sp", "tp"), P(None, "tp"), P())
    return jax.shard_map(local, mesh=mesh, in_specs=in_specs, out_specs=out_specs, check_vma=False)
```

```python
import jax
import jax.numpy as jnp
from jax import lax
from jax.experimental import pallas as pl
from jax.experimental.pallas import tpu as pltpu
from jax.sharding import PartitionSpec as P


HEAD_DIM = 128
SEG = 64
LEFT = 4
MAX_REL = 128
ENTRIES = MAX_REL + SEG
EPSILON = 1e-06
FACTOR = HEAD_DIM ** (-0.5)
TAIL = LEFT * SEG

BLOCK = 2 * SEG
WINDOW = LEFT // 2 + 1
PREV = WINDOW - 1
MASKED = -1e30

F32 = jnp.float32
BF16 = jnp.bfloat16


def dot(a, b, contract):
    return lax.dot_general(a, b, ((contract[:1], contract[1:]), ((), ())), preferred_element_type=F32)


def shifted(block, distance):
    size = lax.axis_size("sp")
    return lax.ppermute(block, "sp", [(i, (i + distance) % size) for i in range(size)])


def unit_rows(rows):
    rows = rows.astype(F32)
    inv_rms = lax.rsqrt(jnp.mean(rows * rows, axis=-1, keepdims=True) + EPSILON)
    return rows * inv_rms, inv_rms


def rows_back(d_normed, unit, inv_rms, gain):
    g = d_normed * gain
    return inv_rms * (g - unit * jnp.mean(g * unit, axis=-1, keepdims=True))


def lanes(shape):
    return lax.broadcasted_iota(jnp.int32, shape, len(shape) - 1)


def toeplitz(row):
    base = pltpu.roll(jnp.broadcast_to(row, (8, 2 * BLOCK)), 0, 1, stride=1, stride_axis=0)
    tiles = [base[:, :BLOCK]]
    for a in range(8, BLOCK, 8):
        tiles.append(pltpu.roll(base, a, 1)[:, :BLOCK])
    return jnp.concatenate(tiles, axis=0)


def diagonals(tile):
    width = 2 * BLOCK
    total = jnp.zeros((8, width), F32)
    empty = jnp.zeros((8, BLOCK), F32)
    for a in range(0, BLOCK, 8):
        part = jnp.concatenate([tile[a : a + 8], empty], axis=1)
        total = total + (pltpu.roll(part, width - a, 1) if a else part)
    out = total[:1]
    for s in range(1, 8):
        out = out + pltpu.roll(total, width - s, 1)[s : s + 1]
    return out


def bias_blocks(table):
    width = 2 * BLOCK
    last = table[:, ENTRIES - 1 :]
    lane = lanes((1, width))
    wide = jnp.concatenate([table, jnp.zeros((1, width - ENTRIES), F32)], axis=1)
    far = jnp.broadcast_to(last, (BLOCK, BLOCK))
    middle = toeplitz(jnp.where(lane < BLOCK, last, pltpu.roll(wide, width - (ENTRIES - 1), 1)))
    near = toeplitz(pltpu.roll(wide, width - (SEG - 1), 1))
    key = lax.broadcasted_iota(jnp.int32, (BLOCK, BLOCK), 0)
    query = lax.broadcasted_iota(jnp.int32, (BLOCK, BLOCK), 1)
    far = jnp.where((key < SEG) & (query >= SEG), MASKED, far)
    near = jnp.where((key >= SEG) & (query < SEG), MASKED, near)
    return [far, middle, near]


def table_row(far, middle, near):
    width = 2 * BLOCK
    lane = lanes((1, width))
    mid = diagonals(middle)
    last = jnp.sum(far) + jnp.sum(jnp.where(lane < BLOCK, mid, 0.0))
    mid = jnp.where(lane < BLOCK, 0.0, mid)
    row = pltpu.roll(diagonals(near), SEG - 1, 1) + pltpu.roll(mid, ENTRIES - 1, 1)
    return row + jnp.where(lane == ENTRIES - 1, last, 0.0)


def add(total, value):
    return value if total is None else total + value


def columns(h):
    return slice(h * HEAD_DIM, (h + 1) * HEAD_DIM)


def block_rows(b):
    return slice(b * BLOCK, (b + 1) * BLOCK)


def pair_lists(blocks):
    pairs = [(p, w) for p in range(blocks) for w in range(WINDOW)]
    return [x for x in pairs if sum(x) < PREV], [x for x in pairs if sum(x) >= PREV]


def own_kernel(
    q_hbm, k_hbm, v_hbm, do_hbm, gains_hbm, table_hbm,
    do_ref, gains_ref, qn_ref, qu_ref, qr_ref, kn_ref, ku_ref, kr_ref, bias_ref, e_ref, dp_ref, stat_ref,
    q_ref, k_ref, v_ref, table_ref, sems,
):
    moves = [(table_hbm, table_ref), (gains_hbm, gains_ref), (q_hbm, q_ref), (k_hbm, k_ref), (v_hbm, v_ref), (do_hbm, do_ref)]
    copies = [pltpu.make_async_copy(a, b, sems.at[i]) for i, (a, b) in enumerate(moves)]
    for copy in copies:
        copy.start()
    for copy in copies:
        copy.wait()
    rows, features = q_ref.shape
    blocks = rows // BLOCK
    _, own = pair_lists(blocks)
    first = lax.axis_index("sp") == 0
    for h in range(features // HEAD_DIM):
        cols = columns(h)
        q_unit, q_rms = unit_rows(q_ref[:, cols])
        k_unit, k_rms = unit_rows(k_ref[:, cols])
        q_norm = (q_unit * gains_ref[0:1]).astype(BF16)
        k_norm = (k_unit * gains_ref[1:2]).astype(BF16)
        qn_ref[:, cols], kn_ref[:, cols] = q_norm, k_norm
        qu_ref[:, cols], ku_ref[:, cols] = q_unit, k_unit
        qr_ref[:, cols] = jnp.broadcast_to(q_rms, q_unit.shape)
        kr_ref[:, cols] = jnp.broadcast_to(k_rms, k_unit.shape)
        bias = bias_blocks(table_ref[h : h + 1])
        for w in range(PREV):
            bias_ref[h, w] = jnp.where(first, MASKED, bias[w])
        for p in range(blocks):
            mine = [(i, w) for i, (pp, w) in enumerate(own) if pp == p]
            keys = slice((p + mine[0][1] - PREV) * BLOCK, (p + 1) * BLOCK)
            at = block_rows(p)
            s = dot(k_norm[keys], q_norm[at], (1, 1)) * FACTOR
            s = s + jnp.concatenate([bias[w] for _, w in mine], axis=0)
            top = jnp.max(s, axis=0, keepdims=True)
            e = jnp.exp(s - top)
            d_prob = dot(v_ref[keys, cols], do_ref[at, cols], (1, 1))
            for n, (i, _) in enumerate(mine):
                e_ref[h, i] = e[block_rows(n)]
                dp_ref[h, i] = d_prob[block_rows(n)]
            stat_ref[h, 2 * p : 2 * p + 1] = top
            stat_ref[h, 2 * p + 1 : 2 * p + 2] = jnp.sum(e, axis=0, keepdims=True)


def keys_kernel(
    pk_ref, qn_ref, do_ref, gains_ref, bias_ref, e_ref, dp_ref, stat_ref,
    pkn_ref, pku_ref, pp_ref, po_ref, both_ref, delta_ref, back_ref, dv_ref,
):
    rows, features = qn_ref.shape
    blocks = rows // BLOCK
    prev, own = pair_lists(blocks)
    heads = features // HEAD_DIM
    cells = [(h, p) for h in range(heads) for p in range(blocks)]
    joined = [(h, p) for h, p in cells if p < PREV]
    k_norm, s, scale = {}, {}, {}
    for h in range(heads):
        k_unit, _ = unit_rows(pk_ref[:, columns(h)])
        k_norm[h] = (k_unit * gains_ref[1:2]).astype(BF16)
        pkn_ref[:, columns(h)], pku_ref[:, columns(h)] = k_norm[h], k_unit
    for h, p in joined:
        s[h, p] = dot(k_norm[h][p * BLOCK :], qn_ref[block_rows(p), columns(h)], (1, 1))
    prob = {}
    for h, p in cells:
        top_own, sum_own = stat_ref[h, 2 * p : 2 * p + 1], stat_ref[h, 2 * p + 1 : 2 * p + 2]
        scale = 1.0
        total = sum_own
        if (h, p) in joined:
            bias = jnp.concatenate([bias_ref[h, w] for w in range(PREV - p)], axis=0)
            scores = s[h, p] * FACTOR + bias
            top = jnp.maximum(top_own, jnp.max(scores, axis=0, keepdims=True))
            e = jnp.exp(scores - top)
            scale = jnp.exp(top_own - top)
            total = sum_own * scale + jnp.sum(e, axis=0, keepdims=True)
        inverse = 1.0 / total
        scale = scale * inverse
        parts = []
        delta = jnp.zeros((1, BLOCK), F32)
        for w in range(WINDOW):
            if p + w < PREV:
                i = prev.index((p, w))
                parts.append(e[block_rows(w)] * inverse)
                pp_ref[h, i] = parts[w]
            else:
                i = own.index((p, w))
                parts.append(e_ref[h, i] * scale)
                po_ref[h, i] = parts[w]
                both = parts[w] * dp_ref[h, i]
                both_ref[h, i] = both
                delta = delta + jnp.sum(both, axis=0, keepdims=True)
        delta_ref[h, p : p + 1] = delta
        prob[h, p] = jnp.concatenate([x.astype(BF16) for x in parts], axis=0)
    dv = [[None] * (blocks + PREV) for _ in range(heads)]
    for h, p in cells:
        dv_w = dot(prob[h, p], do_ref[block_rows(p), columns(h)], (1, 0))
        for w in range(WINDOW):
            dv[h][p + w] = add(dv[h][p + w], dv_w[block_rows(w)])
    for h in range(heads):
        for b in range(PREV):
            back_ref[block_rows(PREV + b), columns(h)] = dv[h][b].astype(BF16)
        for b in range(blocks):
            dv_ref[block_rows(b), columns(h)] = dv[h][PREV + b]


def values_kernel(
    pv_ref, pp_ref, po_ref, both_ref, delta_ref, do_ref, qn_ref, kn_ref, pkn_ref, qu_ref, ku_ref, pku_ref, _,
    dq_ref, back_ref, dk_ref, parts_ref,
):
    rows, features = qn_ref.shape
    heads = features // HEAD_DIM
    blocks = rows // BLOCK
    prev, own = pair_lists(blocks)
    cells = [(h, p) for h in range(heads) for p in range(blocks)]
    d_score, d_low, pieces = {}, {}, []
    new = {}
    for h, p in cells:
        if any(pp == p for pp, _ in prev):
            new[h, p] = dot(pv_ref[p * BLOCK :, columns(h)], do_ref[block_rows(p), columns(h)], (1, 1))
    for h, p in cells:
        delta = delta_ref[h, p : p + 1]
        d_score[h, p] = [None] * WINDOW
        for w in range(WINDOW):
            if p + w < PREV:
                d_prob = new[h, p][block_rows(w)]
                delta = delta + jnp.sum(pp_ref[h, prev.index((p, w))] * d_prob, axis=0, keepdims=True)
        for w in range(WINDOW):
            if p + w < PREV:
                d_score[h, p][w] = pp_ref[h, prev.index((p, w))] * (new[h, p][block_rows(w)] - delta)
            else:
                i = own.index((p, w))
                d_score[h, p][w] = both_ref[h, i] - po_ref[h, i] * delta
        d_low[h, p] = jnp.concatenate([d.astype(BF16) for d in d_score[h, p]], axis=0)
    dk = [[None] * (blocks + PREV) for _ in range(heads)]
    for h, p in cells:
        dk_w = dot(d_low[h, p], qn_ref[block_rows(p), columns(h)], (1, 0))
        for w in range(WINDOW):
            dk[h][p + w] = add(dk[h][p + w], dk_w[block_rows(w)])
    d_gain_q = jnp.zeros((1, HEAD_DIM), F32)
    d_gain_k = jnp.zeros((1, HEAD_DIM), F32)
    for h, p in cells:
        at, cols = block_rows(p), columns(h)
        k_w = [pkn_ref[block_rows(e), cols] if e < PREV else kn_ref[block_rows(e - PREV), cols] for e in range(p, p + WINDOW)]
        dq = dot(d_low[h, p], jnp.concatenate(k_w, axis=0), (0, 0)) * FACTOR
        d_gain_q = d_gain_q + jnp.sum(dq * qu_ref[at, cols], axis=0, keepdims=True)
        dq_ref[at, cols] = dq
    for h in range(heads):
        band = [sum(d_score[h, p][w] for p in range(blocks)) for w in range(WINDOW)]
        row = table_row(*band)
        pieces.append(row[:, :ENTRIES])
    for h in range(heads):
        cols = columns(h)
        for b in range(blocks + PREV):
            d_here = dk[h][b] * FACTOR
            if b < PREV:
                unit = pku_ref[block_rows(b), cols]
                back_ref[block_rows(b), cols] = d_here.astype(BF16)
            else:
                unit = ku_ref[block_rows(b - PREV), cols]
                dk_ref[block_rows(b - PREV), cols] = d_here
            d_gain_k = d_gain_k + jnp.sum(d_here * unit, axis=0, keepdims=True)
    gap = -heads * ENTRIES % HEAD_DIM
    pieces += ([jnp.zeros((1, gap), F32)] if gap else []) + [d_gain_q, d_gain_k]
    flat = jnp.concatenate(pieces, axis=1)
    lines = [flat[:, c : c + HEAD_DIM] for c in range(0, flat.shape[1], HEAD_DIM)]
    once = jnp.concatenate(lines * 8, axis=0)
    for r in range(0, parts_ref.shape[0], once.shape[0]):
        parts_ref[r : r + once.shape[0]] = once


def final_kernel(
    dq_ref, dk_ref, dv_ref, back_ref, qu_ref, qr_ref, ku_ref, kr_ref, gains_ref, parts_ref,
    dq_out, dk_out, dv_out, dt_ref, dg_ref,
):
    rows, features = dk_ref.shape
    heads = features // HEAD_DIM
    tp = lax.axis_size("tp")
    for h in range(heads):
        cols = columns(h)
        for b in range(rows // BLOCK):
            at = block_rows(b)
            dq_out[at, cols] = rows_back(
                dq_ref[at, cols], qu_ref[at, cols], qr_ref[at, cols], gains_ref[0:1]
            ).astype(BF16)
            dk, dv = dk_ref[at, cols], dv_ref[at, cols]
            from_end = b - (rows - TAIL) // BLOCK
            if from_end >= 0:
                dk = dk + back_ref[block_rows(from_end), cols].astype(F32)
                dv = dv + back_ref[block_rows(PREV + from_end), cols].astype(F32)
            dk_out[at, cols] = rows_back(dk, ku_ref[at, cols], kr_ref[at, cols], gains_ref[1:2]).astype(BF16)
            dv_out[at, cols] = dv.astype(BF16)
    lines = -(-heads * ENTRIES // HEAD_DIM) + 2
    width = lines * HEAD_DIM
    each, group = parts_ref.shape[0] // tp, 8 * lines
    sums = []
    for i in range(tp):
        fold = parts_ref[i * each : i * each + group]
        for r in range(group, each, group):
            fold = fold + parts_ref[i * each + r : i * each + r + group]
        rows_of = [sum(fold[n : n + 1] for n in range(c, group, lines)) for c in range(lines)]
        sums.append(jnp.concatenate(rows_of, axis=1))
    mine, total = sums[0], sums[0]
    for i in range(1, tp):
        mine = jnp.where(lax.axis_index("tp") == i, sums[i], mine)
        total = total + sums[i]
    for h in range(heads):
        dt_ref[h : h + 1, :] = mine[:, h * ENTRIES : (h + 1) * ENTRIES]
    dg_ref[0:1] = total[:, width - 2 * HEAD_DIM : width - HEAD_DIM]
    dg_ref[1:2] = total[:, width - HEAD_DIM :]


def call(kernel, name, outs, *operands, **options):
    place = jax.ShapeDtypeStruct if name == "final" else pltpu.VMEM
    return pl.pallas_call(
        kernel,
        out_shape=tuple(place(*o) for o in outs),
        **options,
        compiler_params=pltpu.CompilerParams(vmem_limit_bytes=12 << 20),
    )(*operands)


def local(queries, keys, values, gains, bias_table, d_out):
    rows, features = queries.shape
    heads = features // HEAD_DIM
    blocks = rows // BLOCK
    prev, own = (len(x) for x in pair_lists(blocks))
    members = lax.axis_size("sp") * lax.axis_size("tp")
    width = (-(-heads * ENTRIES // HEAD_DIM) + 2) * HEAD_DIM
    wide, low = ((rows, features), F32), ((rows, features), BF16)
    tail, tail_low = ((TAIL, features), F32), ((TAIL, features), BF16)
    tiles = lambda n: ((heads, n, BLOCK, BLOCK), F32)

    prev_k = shifted(keys[rows - TAIL :], 1)
    prev_v = shifted(values[rows - TAIL :], 1)
    do, g, qn, qu, qr, kn, ku, kr, bias, e_own, dp_own, stats = call(
        own_kernel, "own",
        (low, ((2, HEAD_DIM), F32), low, wide, wide, low, wide, wide, tiles(PREV), tiles(own), tiles(own),
         ((heads, 2 * blocks, BLOCK), F32)),
        *(pltpu.with_memory_space_constraint(x, pltpu.HBM) for x in (queries, keys, values, d_out, gains, bias_table.T)),
        in_specs=[pl.BlockSpec(memory_space=pltpu.HBM)] * 6,
        scratch_shapes=[pltpu.VMEM(*low)] * 3
        + [pltpu.VMEM((heads, ENTRIES), F32), pltpu.SemaphoreType.DMA((6,))],
    )
    pkn, pku, p_prev, p_own, both, delta_own, back_v, dv_own = call(
        keys_kernel, "keys", (tail_low, tail, tiles(prev), tiles(own), tiles(own), ((heads, blocks, BLOCK), F32), ((2 * TAIL, features), BF16), wide),
        prev_k, qn, do, g, bias, e_own, dp_own, stats,
    )
    dq, back, dk_own, parts = call(
        values_kernel, "values", (wide, ((2 * TAIL, features), BF16), wide, ((members * width // HEAD_DIM, HEAD_DIM), F32)),
        prev_v, p_prev, p_own, both, delta_own, do, qn, kn, pkn, qu, ku, pku, back_v, input_output_aliases={12: 1},
    )
    back = shifted(back, -1)
    parts = lax.all_to_all(parts.reshape(members, 1, width), ("tp", "sp"), 0, 0)
    parts = parts.reshape(members * width // HEAD_DIM, HEAD_DIM)
    d_queries, d_keys, d_values, d_table, d_gains = call(
        final_kernel, "final", (low, low, low, ((heads, ENTRIES), F32), ((2, HEAD_DIM), F32)),
        dq, dk_own, dv_own, back, qu, qr, ku, kr, g, parts,
    )
    return d_queries, d_keys, d_values, d_table.T, d_gains


def solution(mesh):
    in_specs = (P("sp", "tp"), P("sp", "tp"), P("sp", "tp"), P(), P(None, "tp"), P("sp", "tp"))
    out_specs = (P("sp", "tp"), P("sp", "tp"), P("sp", "tp"), P(None, "tp"), P())
    return jax.shard_map(local, mesh=mesh, in_specs=in_specs, out_specs=out_specs, check_vma=False)
```
